256 devices in a mesh: sp: 64 (over z, y, core), tp: 4 (over x).
Axes of the slice: x: 4, y: 4, z: 8, core: 2. Of those that a mesh axis runs over, the one named last changes fastest.
Arguments:
- stream: bfloat16 [32768, 2048], P(('sp', 'tp')), may hold values from -6 to 6
- conv_value: bfloat16 [32768, 512], P('sp', 'tp'), may hold values from -6 to 6
- conv_gate: bfloat16 [32768, 512], P('sp', 'tp'), may hold values from -8 to 8
- doc_ids: int32 [32768], P('sp'), may hold values from 0 to 31, never falling along the last dimension, each value on 1 to 2048 neighbouring positions
- conv_taps: float32 [31, 512], P(None, 'tp'), may hold values from -2.2 to 2.2
- conv_bias: float32 [512], P('tp'), may hold values from -3 to 3
- chan_gain: float32 [512], replicated, may hold values from 0.1 to 1.9
- chan_shift: float32 [512], replicated, may hold values from -3 to 3
- out_weight: bfloat16 [512, 2048], replicated, may hold values from -0.25 to 0.25
- rms_gain: float32 [2048], replicated, may hold values from 0.1 to 1.9
- expert_ids: int32 [32768, 2], P(('sp', 'tp')), may hold values from 0 to 127, all different within a row; in each aligned block of 128 rows (0 to 127, 128 to 255, ...) at most 3 rows name the same one
- group_prob: float32 [32768], P(('sp', 'tp')), may hold values from 0.3 to 1
- route_logits: float32 [32768, 2], P(('sp', 'tp')), may hold values from -6 to 6
- expert_gate: bfloat16 [128, 2048, 1024], P('sp', None, 'tp'), may hold values from -0.125 to 0.125
- expert_up: bfloat16 [128, 2048, 1024], P('sp', None, 'tp'), may hold values from -0.125 to 0.125
- expert_down: bfloat16 [128, 1024, 2048], P('sp', 'tp'), may hold values from -0.1875 to 0.1875
Outputs:
- mixed: bfloat16 [32768, 2048], P(('sp', 'tp'))
The draws below stay inside these ranges and needn't reach their ends.
Inputs may be any that keep to these rules, and one draw needn't show every extreme that they name: `expert_ids`: each row names 2 different experts. In each aligned block of 128 rows (the rows of one device) no expert is named by more than 3 rows, a bound that some block reaches. `doc_ids`: document numbers never fall along the sequence; every document has 1 to 2048 positions, one exactly 2048.
All inputs are finite; a program needn't handle non-finite values.
Results may differ from the reference program's by a relative error of at most 0.012.
Values may be sent and summed in bfloat16 or wider, within the bound.
A program may use at most 64 MiB of HBM per device.

```python
import math
import jax
import jax.numpy as jnp
import numpy as np
from jax import lax

D = 2048
CONV_CH = 512
FF = 1024
WIDTH = 31
TOPK = 2
TOK_DEV = 128
EXPERTS = 128
CAP = 3
TOKENS = 32768
DOCS = 32
DOC_MOST = 2048
N_TP = 4


def draw_conv_taps(key, part):
    first, second, third = jax.random.split(jax.random.fold_in(key, 11), 3)
    base = jnp.clip(jax.random.normal(first, (WIDTH, CONV_CH), jnp.float32), -4.0, 4.0)
    levels = jnp.exp(jax.random.uniform(second, (4,), jnp.float32, -1.2, 1.2))
    column = jnp.repeat(levels, CONV_CH // 4)
    jitter = jax.random.uniform(third, (CONV_CH,), jnp.float32, 0.7, 1.0)
    taps = base * (column * jitter)[None, :] * WIDTH ** (-0.5)
    return jnp.clip(taps, -2.2, 2.2)


def steps_of(rng, dims, shards, low, high):
    loudness, own = 1.0, jax.random.fold_in(rng, 6)
    for position, blocks in shards:
        heights = jnp.exp(jax.random.uniform(jax.random.fold_in(own, position), (blocks,), jnp.float32, low / len(shards), high / len(shards)))
        loudness = loudness * jnp.repeat(heights, dims[position] // blocks).reshape([-1 if axis == position else 1 for axis in range(len(dims))])
    return loudness


def split_up(amount, total, limit, slope):
    loads = [(1 << 20) // math.isqrt(standing ** slope) + 1 for standing in range(2, amount + 1)]
    spare, holding = total - limit - (amount - 1), [1] * (amount - 1)
    while spare > 0:
        free = [i for i in range(amount - 1) if holding[i] < limit]
        pool, budget = sum([loads[i] for i in free]), spare
        for i in free:
            more = min(limit - holding[i], max(1, budget * loads[i] // pool), spare)
            holding[i] = holding[i] + more
            spare = spare - more
    return np.array([limit] + holding)


def ragged_sizes(own_key, number_of, total, most, lean):
    if number_of == 2:
        one = jax.random.randint(own_key, (), max(1, total - most), min(most, total - 1) + 1)
        return jnp.stack([one, total - one])
    tallies = jnp.asarray(split_up(number_of, total, most, lean), jnp.int32)
    pairs = (number_of - 1) // 2
    source_of, taker = tallies[1:1 + 2 * pairs:2], tallies[2:2 + 2 * pairs:2]
    margin = jnp.minimum(source_of - 1, most - taker)
    passed = jax.random.randint(jax.random.fold_in(own_key, 1), (pairs,), 0, 1 << 20) % (margin + 1)
    tallies = tallies.at[1:1 + 2 * pairs:2].set(source_of - passed).at[2:2 + 2 * pairs:2].set(taker + passed)
    return tallies[jax.random.permutation(jax.random.fold_in(own_key, 2), number_of)]


def shared_out(own_key, own, number, rows, count, top, limit, lean):
    order = jax.random.permutation(own_key, count)
    heavy_load, ordinary = portions_of(count, rows * top, limit, lean, True), portions_of(count, rows * top, limit, lean, False)
    places = jnp.arange(count)

    def named(tallies, turn):
        used = int((tallies > 0).sum())
        fixed = max(1, used // 4)
        moved = fixed + (places - fixed + turn * (used - fixed)) % max(1, count - fixed)
        return jnp.zeros((count,), jnp.int32).at[order[jnp.where(places < fixed, places, moved)]].set(jnp.asarray(tallies, jnp.int32))

    tallies = jnp.where(number % 4 == 0, named(heavy_load, number // 4), named(ordinary, number - number // 4 - 1))
    mixed = jax.random.permutation(jax.random.fold_in(own, 3), count)
    giver, taker = mixed[0:count // 2 * 2:2], mixed[1:count // 2 * 2:2]
    room = jnp.minimum(tallies[giver] - 1, limit - tallies[taker]) // 2
    room = jnp.where((giver == order[0]) | (taker == order[0]) | (tallies[taker] == 0), 0, jnp.maximum(room, 0))
    moved = jax.random.randint(jax.random.fold_in(own, 4), (count // 2,), 0, 1 << 20) % (room + 1)
    tallies = tallies.at[giver].add(-moved).at[taker].add(moved)
    items = jnp.searchsorted(jnp.cumsum(tallies), jnp.arange(rows * top), side="right").astype(jnp.int32)
    listing = items.reshape(top, rows).T
    listing = listing[jax.random.permutation(jax.random.fold_in(own, 1), rows)]
    turn = jax.random.randint(jax.random.fold_in(own, 2), (rows, 1), 0, top)
    return jnp.take_along_axis(listing, (jnp.arange(top)[None, :] + turn) % top, axis=1)


def portions_of(count, total, most, slope, full):
    portions = [(1 << 20) // math.isqrt(rank ** slope) + 1 for rank in range(1, count + 1)]
    largest = most if full else min(most, max(-(-total // count), total * portions[0] // sum(portions)))
    least = 1 if total - largest >= count - 1 else 0
    given, spare = [largest] + [least] * (count - 1), total - largest - least * (count - 1)
    while spare > 0:
        movable = [i for i in range(1, count) if given[i] < largest] or [i for i in range(1, count) if given[i] < most]
        mass, left = sum([portions[i] for i in movable]), spare
        for i in movable:
            more = min(most - given[i], max(1, left * portions[i] // mass), spare)
            given[i] = given[i] + more
            spare = spare - more
    return np.array(given)


def gaussian(rng, dims, deviation, most, cuts=(), kind=jnp.bfloat16):
    values = deviation * jax.random.normal(rng, dims, jnp.float32)
    if cuts:
        values = values * steps_of(rng, dims, cuts, -0.22, 0.18)
    return jnp.clip(values, -most, most).astype(kind)


def setup_inputs(seed: int = 0) -> dict:
    seeds = jax.random.split(jax.random.key(seed), 17)
    stream = gaussian(seeds[0], (TOKENS, D), 1.0, 6.0, ((0, 256),))
    conv_value = gaussian(seeds[1], (TOKENS, CONV_CH), 1.0, 6.0, ((0, 64), (1, 4)))
    conv_gate = gaussian(seeds[2], (TOKENS, CONV_CH), 1.5, 8.0, ((0, 64), (1, 4)))
    doc_ids = jnp.searchsorted(jnp.cumsum(ragged_sizes(seeds[3], DOCS, TOKENS, DOC_MOST, 0)), jnp.arange(TOKENS), side="right").astype(jnp.int32)
    conv_taps = draw_conv_taps(jax.random.fold_in(seeds[16], 71), 0)
    conv_bias = gaussian(seeds[5], (CONV_CH,), 0.5, 3.0, ((0, 4),), jnp.float32)
    chan_gain = jnp.clip(1.0 + 0.18 * jax.random.normal(seeds[6], (CONV_CH,), jnp.float32), 0.1, 1.9)
    chan_shift = gaussian(seeds[7], (CONV_CH,), 0.5, 3.0, (), jnp.float32)
    out_weight = gaussian(seeds[8], (CONV_CH, D), CONV_CH ** -0.5, 0.25)
    rms_gain = jnp.clip(1.0 + 0.18 * jax.random.normal(seeds[9], (D,), jnp.float32), 0.1, 1.9)
    expert_ids_keys = jax.random.split(jax.random.fold_in(seeds[10], 1), TOKENS // TOK_DEV)
    expert_ids_turns = jax.random.permutation(jax.random.fold_in(seeds[10], 3), TOKENS // TOK_DEV)
    expert_ids = jax.vmap(lambda own, number: shared_out(jax.random.fold_in(seeds[10], 2), own, number, TOK_DEV, EXPERTS, TOPK, CAP, 1))(expert_ids_keys, expert_ids_turns).reshape((TOKENS, TOPK))
    group_prob = jnp.clip(0.3 + 0.7 * jax.random.uniform(seeds[11], (TOKENS,), jnp.float32) ** steps_of(seeds[11], (TOKENS,), ((0, 256),), -0.2, 0.2), 0.3, 1.0)
    route_logits = gaussian(seeds[12], (TOKENS, TOPK), 1.5, 6.0, ((0, 256),), jnp.float32)
    expert_gate = gaussian(seeds[13], (EXPERTS, D, FF), D ** -0.5, 0.125, ((0, 64), (2, 4)))
    expert_up = gaussian(seeds[14], (EXPERTS, D, FF), D ** -0.5, 0.125, ((0, 64), (2, 4)))
    expert_down = gaussian(seeds[15], (EXPERTS, FF, D), FF ** -0.5, 0.1875, ((0, 64), (1, 4)))
    return dict(stream=stream, conv_value=conv_value, conv_gate=conv_gate, doc_ids=doc_ids, conv_taps=conv_taps, conv_bias=conv_bias, chan_gain=chan_gain, chan_shift=chan_shift, out_weight=out_weight, rms_gain=rms_gain, expert_ids=expert_ids, group_prob=group_prob, route_logits=route_logits, expert_gate=expert_gate, expert_up=expert_up, expert_down=expert_down)


eps = 1e-06
row_block = 128

def causal_conv(values, gates, docs, conv_taps, conv_bias):
    reach = conv_taps.shape[0] - 1
    acts = values.astype(jnp.float32) * jax.nn.sigmoid(gates.astype(jnp.float32))
    total = values.shape[0] - reach
    result = jnp.broadcast_to(conv_bias[None, :], (total, values.shape[1])).astype(jnp.float32)
    own_doc = docs[reach:]
    for offset in range(reach + 1):
        begin = reach - offset
        same = (docs[begin:begin + total] == own_doc)[:, None]
        result = result + jnp.where(same, acts[begin:begin + total], 0.0) * conv_taps[offset][None, :]
    return result.astype(jnp.bfloat16)

def channel_norm(conved, chan_gain, chan_shift):
    values = conved.astype(jnp.float32)
    mean = lax.optimization_barrier(jnp.mean(values, axis=-1, keepdims=True))
    square = lax.optimization_barrier(jnp.mean(values * values, axis=-1, keepdims=True))
    spread = square - mean * mean
    scaled = (values - mean) * lax.rsqrt(spread + eps) * chan_gain + chan_shift
    return jax.nn.silu(scaled).astype(jnp.bfloat16)

def rms_norm(resid, rms_gain):
    values = resid.astype(jnp.float32)
    square = lax.optimization_barrier(jnp.mean(values * values, axis=-1, keepdims=True))
    return (values * lax.rsqrt(square + eps) * rms_gain).astype(jnp.bfloat16)

def route_weights(group_prob, route_logits):
    gap = route_logits[:, 0] - route_logits[:, 1]
    return jnp.stack([group_prob * jax.nn.sigmoid(gap), group_prob * jax.nn.sigmoid(-gap)], axis=1)

def run_experts(normed, expert_ids, expert_gate, expert_up, expert_down):
    routes = TOKENS * TOPK
    expert = expert_ids.reshape(routes).astype(jnp.int32)
    token = (jnp.arange(routes, dtype=jnp.int32) // TOPK).astype(jnp.int32)
    order = jnp.argsort(expert, stable=True).astype(jnp.int32)
    sorted_expert = expert[order]
    sorted_token = token[order]
    counts = lax.optimization_barrier(jnp.sum((expert[:, None] == jnp.arange(EXPERTS, dtype=jnp.int32)[None, :]).astype(jnp.int32), axis=0))
    begin = jnp.cumsum(counts) - counts
    padded = (counts + row_block - 1) // row_block * row_block
    pad_end = jnp.cumsum(padded)
    pad_begin = pad_end - padded
    dest = (pad_begin[sorted_expert] + jnp.arange(routes, dtype=jnp.int32) - begin[sorted_expert]).astype(jnp.int32)
    n_rows = (routes + row_block - 1) // row_block * row_block + EXPERTS * row_block
    n_blocks = n_rows // row_block
    row_token = jnp.zeros((n_rows,), jnp.int32).at[dest].set(sorted_token)
    starts = jnp.arange(n_blocks, dtype=jnp.int32) * row_block
    block_expert = jnp.minimum(lax.optimization_barrier(jnp.sum((pad_end[None, :] <= starts[:, None]).astype(jnp.int32), axis=1)), EXPERTS - 1).astype(jnp.int32)
    quarter = FF // N_TP

    def run_block(inputs):
        rows, index = inputs
        picked = normed[rows]
        gated = jnp.dot(picked, expert_gate[index], preferred_element_type=jnp.float32)
        upward = jnp.dot(picked, expert_up[index], preferred_element_type=jnp.float32)
        hidden = (jax.nn.silu(gated) * upward).astype(jnp.bfloat16)
        pieces = hidden.reshape(row_block, N_TP, quarter).astype(jnp.float32)
        downs = expert_down[index].reshape(N_TP, quarter, D).astype(jnp.float32)
        partial_value = jnp.einsum('rqf,qfd->qrd', pieces, downs).astype(jnp.bfloat16)
        return lax.optimization_barrier(jnp.sum(partial_value.astype(jnp.float32), axis=0)).astype(jnp.bfloat16)
    outputs = lax.map(run_block, (row_token.reshape(n_blocks, row_block), block_expert)).reshape(n_rows, D)
    slot = jnp.zeros((routes,), jnp.int32).at[order].set(dest)
    return outputs[slot]

def reference(stream, conv_value, conv_gate, doc_ids, conv_taps, conv_bias, chan_gain, chan_shift, out_weight, rms_gain, expert_ids, group_prob, route_logits, expert_gate, expert_up, expert_down):
    reach = WIDTH - 1
    values = jnp.concatenate([jnp.zeros((reach, CONV_CH), jnp.bfloat16), conv_value], axis=0)
    gates = jnp.concatenate([jnp.zeros((reach, CONV_CH), jnp.bfloat16), conv_gate], axis=0)
    docs = jnp.concatenate([jnp.full((reach,), -1, jnp.int32), doc_ids.astype(jnp.int32)], axis=0)
    conved = causal_conv(values, gates, docs, conv_taps, conv_bias)
    activated = channel_norm(conved, chan_gain, chan_shift)
    projected = jnp.dot(activated, out_weight, preferred_element_type=jnp.float32)
    resid = (stream.astype(jnp.float32) + projected).astype(jnp.bfloat16)
    normed = rms_norm(resid, rms_gain)
    weights = route_weights(group_prob, route_logits)
    routed = run_experts(normed, expert_ids, expert_gate, expert_up, expert_down)
    combined = lax.optimization_barrier(jnp.sum(weights[:, :, None] * routed.reshape(TOKENS, TOPK, D).astype(jnp.float32), axis=1))
    return (resid.astype(jnp.float32) + combined).astype(jnp.bfloat16)
```

```python
import functools

import jax
import jax.numpy as jnp
from jax import lax
from jax.experimental import pallas as pl
from jax.experimental.pallas import tpu as pltpu
from jax.sharding import PartitionSpec as P

eps = 1e-06
MESH = pl.DeviceIdType.MESH
NX = 4
CORES = 2
SUB = 16


def passed_along(x, axis, by):
    size = lax.axis_size(axis)
    pairs = [(i, i + by) for i in range(size) if 0 <= i + by < size]
    return lax.ppermute(x, axis, pairs)


def causal_conv(values, gates, docs, conv_taps, conv_bias):
    reach = conv_taps.shape[0] - 1
    acts = values.astype(jnp.float32) * jax.nn.sigmoid(gates.astype(jnp.float32))
    total = values.shape[0] - reach
    result = jnp.broadcast_to(conv_bias[None, :], (total, values.shape[1]))
    own_doc = docs[reach:]
    for offset in range(reach + 1):
        begin = reach - offset
        same = (docs[begin : begin + total] == own_doc)[:, None]
        result = (
            result + jnp.where(same, acts[begin : begin + total], 0.0) * conv_taps[offset][None, :]
        )
    return result.astype(jnp.bfloat16)


def finish_norm(values, mean, square, gain, shift):
    spread = square - mean * mean
    scaled = (values - mean) * lax.rsqrt(spread + eps) * gain + shift
    return jax.nn.silu(scaled).astype(jnp.bfloat16)


def silu(v):
    return v / (1.0 + jnp.exp(-v))


def expert_kernel(
    ny,
    nz,
    cap,
    src_idx,
    slot_idx,
    wts,
    normed,
    resid,
    gate,
    up,
    down,
    out,
    outg,
    own,
    par,
    stage,
    xbuf,
    wg,
    wu,
    wd,
    acc,
    psend,
    precv,
    rsend,
    ret,
    w_send,
    w_recv,
    a_send,
    a_recv,
    f_send,
    f_recv,
    p_send,
    p_recv,
    r_send,
    r_recv,
):
    sp = lax.axis_index("sp")
    x = lax.axis_index("tp")
    core = sp % CORES
    ring = sp // CORES
    y = ring % ny
    z = ring // ny
    per = nz * 2 * CORES
    rows = per * cap
    wide = rows * SUB
    experts = ny * nz * NX

    def place(zz, yy, cc):
        return (zz * ny + yy) * CORES + cc

    def weight_copies(l):
        j = CORES * core + l
        d = (x - j + NX) % NX
        slot = d // 2
        to_core = ((d + 1) // 2) % 2
        to_x = (j + to_core) % NX
        return d, slot, to_core, to_x

    triples = ((gate, wg), (up, wu), (down, wd))
    for l in range(2):
        d, slot, to_core, to_x = weight_copies(l)
        mine = d == core

        @pl.when(mine)
        def _():
            for a, (src, dst) in enumerate(triples):
                pltpu.make_async_copy(src.at[l], dst.at[slot], w_recv.at[slot, a]).start()

        @pl.when(jnp.logical_not(mine))
        def _():
            for a, (src, dst) in enumerate(triples):
                pltpu.make_async_remote_copy(
                    src_ref=src.at[l],
                    dst_ref=dst.at[slot],
                    send_sem=w_send.at[l, a],
                    recv_sem=w_recv.at[slot, a],
                    device_id=(ring * CORES + to_core, to_x),
                    device_id_type=MESH,
                ).start()

    def fill(i, carry):
        outg[i] = normed[src_idx[i]]
        return carry

    lax.fori_loop(0, experts * cap, fill, 0, unroll=8)

    my_j = (x - core + NX) % NX
    my_e = ring * NX + my_j

    own[0, pl.ds(core * cap, cap)] = outg[pl.ds(my_e * cap, cap)]

    def send_rows(i, carry):
        dy = i // (nz * NX)
        dz = (i // NX) % nz
        dd = (core + i) % NX
        j = (x - dd + NX) % NX
        p = dd // 2
        m = ((dd + 1) // 2) % 2
        to_ring = ((z + dz) % nz) * ny + (y + dy) % ny
        e = to_ring * NX + j
        slot = (dz * 2 + p) * CORES + core
        pltpu.make_async_remote_copy(
            src_ref=outg.at[pl.ds(e * cap, cap)],
            dst_ref=own.at[dy, pl.ds(slot * cap, cap)],
            send_sem=a_send,
            recv_sem=a_recv.at[dy],
            device_id=(to_ring * CORES + m, (j + m) % NX),
            device_id_type=MESH,
        ).start()
        return carry

    lax.fori_loop(1, experts, send_rows, 0)

    mate = (ring * CORES + 1 - core, (x + 1 - 2 * core + NX) % NX)

    def forward(g):
        return pltpu.make_async_remote_copy(
            src_ref=own.at[g],
            dst_ref=par.at[g],
            send_sem=f_send.at[g],
            recv_sem=f_recv.at[g],
            device_id=mate,
            device_id_type=MESH,
        )

    def partial_copy(g):
        return pltpu.make_async_remote_copy(
            src_ref=psend.at[g],
            dst_ref=precv.at[g],
            send_sem=p_send.at[g],
            recv_sem=p_recv.at[g],
            device_id=mate,
            device_id_type=MESH,
        )

    def arrive(g):
        @pl.when(g == 0)
        def _():
            part = own.at[0, pl.ds(0, rows - cap)]
            pltpu.make_async_copy(part, part, a_recv.at[0]).wait()

        @pl.when(g > 0)
        def _():
            pltpu.make_async_copy(own.at[g], own.at[g], a_recv.at[g]).wait()

        forward(g).start()

    def load_rows(buf, g, base):
        stage[...] = buf[g].reshape(wide, 128).astype(jnp.float32)
        for s in range(SUB):
            piece = stage[pl.ds(s, rows, stride=SUB), :]
            xbuf[pl.ds(base, rows), pl.ds(s * 128, 128)] = piece.astype(jnp.bfloat16)

    def compute(g):
        load_rows(own, g, 0)
        forward(g).wait_recv()
        load_rows(par, g, rows)
        x_all = xbuf[...]
        hidden = []
        for q in range(2):
            gated = jnp.dot(x_all, wg[q], preferred_element_type=jnp.float32)
            upward = jnp.dot(x_all, wu[q], preferred_element_type=jnp.float32)
            hidden.append((silu(gated) * upward).astype(jnp.bfloat16))
        total = jnp.dot(hidden[0], wd[0], preferred_element_type=jnp.float32) + jnp.dot(
            hidden[1], wd[1], preferred_element_type=jnp.float32
        )
        acc[g % 2] = total[:rows]
        psend[g] = total[rows:].astype(jnp.bfloat16)
        partial_copy(g).start()

    def finish(g):
        partial_copy(g).wait_recv()
        for s in range(SUB):
            cols = pl.ds(s * 128, 128)
            whole = acc[g % 2, :, cols] + precv[g, :, cols].astype(jnp.float32)
            stage[pl.ds(s, rows, stride=SUB), :] = whole
        rsend[g] = stage[...].astype(jnp.bfloat16).reshape(rows, SUB, 128)

        def send_back(i, carry):
            s = (core + i) % per
            from_core = s % CORES
            p = (s // CORES) % 2
            dz = s // (2 * CORES)
            dd = core + p * (3 - 2 * core)
            t = (my_j + dd) % NX
            to_sp = place((z - dz + nz) % nz, (y - g + ny) % ny, from_core)
            pltpu.make_async_remote_copy(
                src_ref=rsend.at[g, pl.ds(s * cap, cap)],
                dst_ref=ret.at[pl.ds(my_e * cap, cap)],
                send_sem=r_send,
                recv_sem=r_recv,
                device_id=(to_sp, t),
                device_id_type=MESH,
            ).start()
            return carry

        @pl.when(g == 0)
        def _():
            ret[pl.ds(my_e * cap, cap)] = rsend[0, pl.ds(core * cap, cap)]
            lax.fori_loop(1, per, send_back, 0)

        @pl.when(g > 0)
        def _():
            lax.fori_loop(0, per, send_back, 0)

    def step(i, carry):
        @pl.when(i < ny)
        def _():
            arrive(i)

        @pl.when(i == 1)
        def _():
            for s in range(2):
                for a, (src, dst) in enumerate(triples):
                    pltpu.make_async_copy(src.at[0], dst.at[s], w_recv.at[s, a]).wait()

        @pl.when(jnp.logical_and(i >= 1, i <= ny))
        def _():
            compute(i - 1)

        @pl.when(i >= 2)
        def _():
            finish(i - 2)

        return carry

    lax.fori_loop(0, ny + 2, step, 0)

    got = ret.at[pl.ds(0, (experts - 1) * cap)]
    pltpu.make_async_copy(got, got, r_recv).wait()

    def combine(t, carry):
        first = ret[slot_idx[2 * t]]
        second = ret[slot_idx[2 * t + 1]]
        mixed = wts[2 * t] * first.astype(jnp.float32) + wts[2 * t + 1] * second.astype(jnp.float32)
        out[t] = (resid[t].astype(jnp.float32) + mixed).astype(jnp.bfloat16)
        return carry

    lax.fori_loop(0, normed.shape[0], combine, 0, unroll=4)

    sent = outg.at[pl.ds(0, (experts - 1) * cap)]
    pltpu.make_async_copy(sent, sent, a_send).wait()
    pltpu.make_async_copy(got, got, r_send).wait()
    for g in range(ny):
        forward(g).wait_send()
        partial_copy(g).wait_send()
    for l in range(2):
        d, slot, to_core, to_x = weight_copies(l)

        @pl.when(d != core)
        def _():
            for a, (src, dst) in enumerate(triples):
                pltpu.make_async_copy(src.at[l], dst.at[slot], w_send.at[l, a]).wait()


def run_experts(ny, nz, cap, src_idx, slot_idx, wts, normed, resid, gate, up, down):
    width = normed.shape[1]
    tokens = normed.shape[0]
    per = nz * 2 * CORES
    rows = per * cap
    experts = ny * nz * NX
    quarter = gate.shape[2]
    bf = jnp.bfloat16
    flat = lambda v: v.reshape(tokens, SUB, width // SUB)
    smem = pl.BlockSpec(memory_space=pltpu.SMEM)
    vmem = pl.BlockSpec(memory_space=pltpu.VMEM)
    hbm = pl.BlockSpec(memory_space=pl.ANY)
    dma = pltpu.SemaphoreType.DMA
    result = pl.pallas_call(
        functools.partial(expert_kernel, ny, nz, cap),
        out_shape=jax.ShapeDtypeStruct((tokens, SUB, width // SUB), bf),
        in_specs=[smem, smem, smem, vmem, vmem, hbm, hbm, hbm],
        out_specs=vmem,
        scratch_shapes=[
            pltpu.VMEM((experts * cap, SUB, 128), bf),
            pltpu.VMEM((ny, rows, SUB, 128), bf),
            pltpu.VMEM((ny, rows, SUB, 128), bf),
            pltpu.VMEM((rows * SUB, 128), jnp.float32),
            pltpu.VMEM((2 * rows, width), bf),
            pltpu.VMEM((2, width, quarter), bf),
            pltpu.VMEM((2, width, quarter), bf),
            pltpu.VMEM((2, quarter, width), bf),
            pltpu.VMEM((2, rows, width), jnp.float32),
            pltpu.VMEM((ny, rows, width), bf),
            pltpu.VMEM((ny, rows, width), bf),
            pltpu.VMEM((ny, rows, SUB, 128), bf),
            pltpu.VMEM((experts * cap, SUB, 128), bf),
            dma((2, 3)),
            dma((2, 3)),
            dma,
            dma((ny,)),
            dma((ny,)),
            dma((ny,)),
            dma((ny,)),
            dma((ny,)),
            dma,
            dma,
        ],
        compiler_params=pltpu.CompilerParams(has_side_effects=True, vmem_limit_bytes=60000 * 1024),
    )(src_idx, slot_idx, wts, flat(normed), flat(resid), gate, up, down)
    return result.reshape(tokens, width)


def body(
    ny,
    nz,
    stream,
    conv_value,
    conv_gate,
    doc_ids,
    conv_taps,
    conv_bias,
    chan_gain,
    chan_shift,
    out_weight,
    rms_gain,
    expert_ids,
    group_prob,
    route_logits,
    expert_gate,
    expert_up,
    expert_down,
):
    reach = conv_taps.shape[0] - 1
    tail_value, tail_gate, tail_doc = passed_along(
        (conv_value[-reach:], conv_gate[-reach:], doc_ids[-reach:]), "sp", 1
    )
    values = jnp.concatenate([tail_value, conv_value], axis=0)
    gates = jnp.concatenate([tail_gate, conv_gate], axis=0)
    docs = jnp.concatenate([tail_doc, doc_ids], axis=0)
    conved = causal_conv(values, gates, docs, conv_taps, conv_bias)
    own_rows = stream.shape[0]
    regrouped = lax.all_to_all(conved, "tp", split_axis=0, concat_axis=1, tiled=True)
    floats = regrouped.astype(jnp.float32)
    mean = jnp.mean(floats, axis=-1, keepdims=True)
    square = jnp.mean(floats * floats, axis=-1, keepdims=True)
    activated = finish_norm(floats, mean, square, chan_gain, chan_shift)
    projected = jnp.dot(activated, out_weight, preferred_element_type=jnp.float32)
    resid = (stream.astype(jnp.float32) + projected).astype(jnp.bfloat16)
    resid_float = resid.astype(jnp.float32)
    mean_square = jnp.mean(resid_float * resid_float, axis=-1, keepdims=True)
    normed = (resid_float * lax.rsqrt(mean_square + eps) * rms_gain).astype(jnp.bfloat16)
    gap = route_logits[:, 0] - route_logits[:, 1]
    weights = jnp.stack(
        [group_prob * jax.nn.sigmoid(gap), group_prob * jax.nn.sigmoid(-gap)], axis=1
    )
    experts_all = lax.axis_size("sp") * expert_gate.shape[0]
    top_count = expert_ids.shape[1]
    cap = 3
    flat_ids = expert_ids.reshape(-1)
    onehot = (flat_ids[:, None] == jnp.arange(experts_all, dtype=jnp.int32)[None, :]).astype(
        jnp.int32
    )
    earlier = jnp.cumsum(onehot, axis=0) - onehot
    ranks = jnp.sum(earlier * onehot, axis=1)
    dest = flat_ids * cap + ranks
    route_token = jnp.arange(flat_ids.shape[0], dtype=jnp.int32) // top_count
    source = jnp.zeros((experts_all * cap,), jnp.int32).at[dest].set(route_token)
    return run_experts(
        ny,
        nz,
        cap,
        source,
        dest,
        weights.reshape(-1),
        normed,
        resid,
        expert_gate,
        expert_up,
        expert_down,
    )


def solution(mesh):
    placed = (
        P(("sp", "tp"), None),
        P("sp", "tp"),
        P("sp", "tp"),
        P("sp"),
        P(None, "tp"),
        P("tp"),
        P(),
        P(),
        P(),
        P(),
        P(("sp", "tp"), None),
        P(("sp", "tp")),
        P(("sp", "tp"), None),
        P("sp", None, "tp"),
        P("sp", None, "tp"),
        P("sp", "tp", None),
    )
    ny = 4
    nz = mesh.shape["sp"] // (ny * CORES)
    return jax.shard_map(
        functools.partial(body, ny, nz),
        mesh=mesh,
        in_specs=placed,
        out_specs=P(("sp", "tp"), None),
        check_vma=False,
    )
```

```python
import functools

import jax
import jax.numpy as jnp
from jax import lax
from jax.experimental import pallas as pl
from jax.experimental.pallas import tpu as pltpu
from jax.sharding import PartitionSpec as P

eps = 1e-06
MESH = pl.DeviceIdType.MESH
NX = 4
CORES = 2
SUB = 16
LANES = 128
HALO = 32
LAG = 2
END_LAG = 4
F32 = jnp.float32
BF = jnp.bfloat16


def silu(v):
    return v / (1.0 + jnp.exp(-v))


def dot(a, b):
    return jnp.dot(a, b, preferred_element_type=F32)


def layer_kernel(
    ny,
    nz,
    cap,
    stream,
    value,
    gatein,
    docs,
    taps,
    bias,
    gain,
    shift,
    out_weight,
    rms_gain,
    ids,
    prob,
    logits,
    gate,
    up,
    down,
    out,
    halo_v,
    halo_g,
    halo_d,
    acts,
    docsb,
    conv,
    regroup,
    actv,
    stream_v,
    ow_v,
    resid,
    stage,
    xbuf,
    combine_w,
    outg,
    own,
    par,
    wg,
    wu,
    wd,
    acc,
    psend,
    precv,
    rsend,
    ret,
    y_sem,
    z_sem,
    l_sem,
    h_send,
    h_recv,
    c_send,
    c_recv,
    w_send,
    w_recv,
    a_send,
    a_recv,
    f_send,
    f_recv,
    p_send,
    p_recv,
    r_send,
    r_recv,
):
    sp = lax.axis_index("sp")
    x = lax.axis_index("tp")
    core = sp % CORES
    ring = sp // CORES
    y = ring % ny
    z = ring // ny
    chunks = 2 * ny
    per = nz * CORES
    rows = per * cap
    experts = ny * nz * NX
    count = ny * nz * CORES
    block = rows_of(conv)
    reach = taps.shape[0] - 1
    width = resid.shape[1]

    def place(zz, yy, cc):
        return (zz * ny + yy) * CORES + cc

    def tell(sem, to):
        pl.semaphore_signal(sem, inc=1, device_id=to, device_id_type=MESH)

    barrier = pltpu.get_barrier_semaphore()
    for dz in range(1, nz):
        tell(barrier, (place((z + dz) % nz, y, core), x))
    for dy in range(1, ny):
        tell(barrier, (place(z, (y + dy) % ny, core), x))
    for dx in range(NX):
        for dc in range(CORES):
            if dx or dc:
                tell(barrier, (ring * CORES + (core + dc) % CORES, (x + dx) % NX))

    @pl.when(sp > 0)
    def _():
        tell(barrier, (sp - 1, x))

    load_ow = pltpu.make_async_copy(out_weight, ow_v, l_sem.at[0])
    load_stream = pltpu.make_async_copy(stream, stream_v, l_sem.at[1])
    load_ow.start()
    load_stream.start()

    tail = value.shape[0] - HALO
    edges = (
        (value.at[pl.ds(tail, HALO)], halo_v),
        (gatein.at[pl.ds(tail, HALO)], halo_g),
        (docs, halo_d),
    )

    def edge_copy(a):
        return pltpu.make_async_remote_copy(
            src_ref=edges[a][0],
            dst_ref=edges[a][1],
            send_sem=h_send.at[a],
            recv_sem=h_recv.at[a],
            device_id=(sp + 1, x),
            device_id_type=MESH,
        )

    triples = ((gate, wg), (up, wu), (down, wd))

    def weight_plan(l):
        j = CORES * core + l
        d = (x - j + NX) % NX
        slot = d // 2
        to_core = ((d + 1) // 2) % 2
        return d, slot, (ring * CORES + to_core, (j + to_core) % NX)

    def weight_piece(l, a, slot):
        src, dst = triples[a // 2]
        half = src.shape[1] // 2
        part = pl.ds(a % 2 * half, half)
        return src.at[l, part], dst.at[slot, part]

    def weight_copy(l, a, slot, to):
        src, dst = weight_piece(l, a, slot)
        return pltpu.make_async_remote_copy(
            src_ref=src,
            dst_ref=dst,
            send_sem=w_send.at[l, a],
            recv_sem=w_recv.at[slot, a],
            device_id=to,
            device_id_type=MESH,
        )

    def start_weights(kinds):
        for a in kinds:
            for l in range(2):
                d, slot, to = weight_plan(l)

                @pl.when(d == core)
                def _():
                    src, dst = weight_piece(l, a, slot)
                    pltpu.make_async_copy(src, dst, w_recv.at[slot, a]).start()

                @pl.when(d != core)
                def _():
                    weight_copy(l, a, slot, to).start()

    line = lax.broadcasted_iota(jnp.int32, (LANES, LANES), 0)
    lane = lax.broadcasted_iota(jnp.int32, (LANES, LANES), 1)
    ones = jnp.ones((LANES, LANES), BF)

    def spread(row):
        return dot(jnp.where(line == lane, row.astype(F32), 0.0).astype(BF), ones)

    def gated(v, g):
        return v.astype(F32) / (1.0 + jnp.exp(-g.astype(F32)))

    acts[pl.ds(HALO, NX * block), :] = gated(value[...], gatein[...])
    for b in range(NX):
        docsb[pl.ds(HALO + b * block, block), :] = spread(docs[pl.ds(b, 1), :])

    def conv_block(b):
        half = block // 2
        for piece in range(2):
            at = HALO + b * block + piece * half
            mine = docsb[pl.ds(at, half), :]
            total = jnp.broadcast_to(bias[...], (half, LANES))
            for j in range(reach + 1):
                same = docsb[pl.ds(at - j, half), :] == mine
                total = total + jnp.where(same, acts[pl.ds(at - j, half), :], 0.0) * taps[
                    pl.ds(j, 1), :
                ]
            conv[b, pl.ds(piece * half, half), :] = total.astype(BF)

    def hand_over(b):
        @pl.when(x == b)
        def _():
            regroup[b] = conv[b]

        @pl.when(x != b)
        def _():
            pltpu.make_async_remote_copy(
                src_ref=conv.at[b],
                dst_ref=regroup.at[x],
                send_sem=c_send,
                recv_sem=c_recv,
                device_id=(sp, b),
                device_id_type=MESH,
            ).start()

    for b in range(1, NX):
        conv_block(b)

    peers = NX * CORES - 1 + ny - 1 + nz - 1

    @pl.when(sp < count - 1)
    def _():
        pl.semaphore_wait(barrier, peers + 1)

    @pl.when(sp == count - 1)
    def _():
        pl.semaphore_wait(barrier, peers)

    @pl.when(sp < count - 1)
    def _():
        for a in range(3):
            edge_copy(a).start()

    for b in range(1, NX):
        hand_over(b)
    for dy in range(1, ny):
        tell(y_sem, (place(z, (y + dy) % ny, core), x))

    @pl.when(sp == 0)
    def _():
        acts[pl.ds(0, HALO), :] = jnp.zeros((HALO, LANES), F32)
        docsb[pl.ds(0, HALO), :] = jnp.full((HALO, LANES), -1.0, F32)

    @pl.when(sp > 0)
    def _():
        for a in range(3):
            edge_copy(a).wait_recv()
        acts[pl.ds(0, HALO), :] = gated(halo_v[...], halo_g[...])
        docsb[pl.ds(0, HALO), :] = spread(halo_d[pl.ds(NX - 1, 1), :])[LANES - HALO :]

    conv_block(0)
    hand_over(0)
    start_weights(range(6))
    pl.semaphore_wait(y_sem, ny - 1)
    for dz in range(1, nz):
        tell(z_sem, (place((z + dz) % nz, y, core), x))

    first = ids[:, 0:1] == lane
    second = ids[:, 1:2] == lane
    match = jnp.where(jnp.logical_or(first, second), 1.0, 0.0)
    rank = dot(jnp.where(lane < line, 1.0, 0.0).astype(BF), match.astype(BF))
    share = jnp.sum(jnp.where(line == lane, prob[...], 0.0), axis=1, keepdims=True)
    gap = logits[:, 0:1] - logits[:, 1:2]
    w_first = share / (1.0 + jnp.exp(-gap))
    w_second = share / (1.0 + jnp.exp(gap))
    w_match = jnp.where(first, w_first, 0.0) + jnp.where(second, w_second, 0.0)
    picks = []
    for r in range(cap):
        at_rank = jnp.where(rank == float(r), match, 0.0)
        picks.append(at_rank.astype(BF))
        weight = at_rank * w_match
        high = weight.astype(BF)
        combine_w[pl.ds(0, block), pl.ds(r * LANES, LANES)] = high
        combine_w[pl.ds(block, block), pl.ds(r * LANES, LANES)] = (
            weight - high.astype(F32)
        ).astype(BF)

    pltpu.make_async_copy(
        regroup.at[pl.ds(0, NX - 1)], regroup.at[pl.ds(0, NX - 1)], c_recv
    ).wait()
    channels = NX * LANES
    parts = [regroup[b].astype(F32) for b in range(NX)]
    mean = jnp.sum(sum(parts[1:], parts[0]), axis=1, keepdims=True) / channels
    squares = [v * v for v in parts]
    square = jnp.sum(sum(squares[1:], squares[0]), axis=1, keepdims=True) / channels
    scale = lax.rsqrt(square - mean * mean + eps)
    for b in range(NX):
        cols = pl.ds(b * LANES, LANES)
        actv[:, cols] = silu((parts[b] - mean) * scale * gain[:, cols] + shift[:, cols]).astype(BF)
    load_ow.wait()
    load_stream.wait()
    summed = (stream_v[...].astype(F32) + dot(actv[...], ow_v[...])).astype(BF)
    resid[...] = summed
    wide = summed.astype(F32)
    power = jnp.sum(wide * wide, axis=1, keepdims=True) / width
    normed = (wide * lax.rsqrt(power + eps) * rms_gain[...]).astype(BF)

    for r in range(cap):
        rows_r = lax.dot_general(
            picks[r], normed, (((0,), (0,)), ((), ())), preferred_element_type=F32
        )
        for s in range(SUB):
            stage[pl.ds(s, experts, stride=SUB), :] = rows_r[:, s * LANES : (s + 1) * LANES]
        outg[:, r] = stage[...].astype(BF).reshape(experts, SUB, LANES)

    my_j = (x - core + NX) % NX
    my_e = ring * NX + my_j

    home = ny - 1
    own[home, core] = outg[my_e]

    def send_rows(g, carry):
        p = g // ny
        to_y = (y + g + 1) % ny
        for dz in range(nz):
            base = ((z + dz) % nz) * ny + to_y
            for k in range(2):
                dd = 2 * p + (core + k) % 2
                j = (x - dd + NX) % NX
                m = ((dd + 1) // 2) % 2

                def start():
                    pltpu.make_async_remote_copy(
                        src_ref=outg.at[base * NX + j],
                        dst_ref=own.at[g, dz * CORES + core],
                        send_sem=a_send,
                        recv_sem=a_recv.at[g],
                        device_id=(base * CORES + m, (j + m) % NX),
                        device_id_type=MESH,
                    ).start()

                if dz == 0 and k == 0:
                    pl.when(g != home)(start)
                else:
                    start()
        return carry

    pl.semaphore_wait(z_sem, nz - 1)
    lax.fori_loop(0, chunks, send_rows, 0)

    mate = (ring * CORES + 1 - core, (x + 1 - 2 * core + NX) % NX)

    def forward(g):
        return pltpu.make_async_remote_copy(
            src_ref=own.at[g],
            dst_ref=par.at[g],
            send_sem=f_send.at[g],
            recv_sem=f_recv.at[g],
            device_id=mate,
            device_id_type=MESH,
        )

    def partial_copy(g):
        return pltpu.make_async_remote_copy(
            src_ref=psend.at[g],
            dst_ref=precv.at[g],
            send_sem=p_send.at[g],
            recv_sem=p_recv.at[g],
            device_id=mate,
            device_id_type=MESH,
        )

    def arrive(g):
        @pl.when(g == home)
        def _():
            part = own.at[home, pl.ds(0, per - 1)]
            pltpu.make_async_copy(part, part, a_recv.at[home]).wait()

        @pl.when(g != home)
        def _():
            pltpu.make_async_copy(own.at[g], own.at[g], a_recv.at[g]).wait()

        forward(g).start()

    def load_rows(buf, g, base):
        stage[pl.ds(0, rows * SUB), :] = buf[g].reshape(rows * SUB, LANES).astype(F32)
        for s in range(SUB):
            piece = stage[pl.ds(s, rows, stride=SUB), :]
            xbuf[pl.ds(base, rows), pl.ds(s * LANES, LANES)] = piece.astype(BF)

    def compute(g):
        load_rows(own, g, 0)
        forward(g).wait_recv()
        load_rows(par, g, rows)
        x_all = xbuf[pl.ds(0, 2 * rows), :]
        hidden = []
        for q in range(2):
            hidden.append((silu(dot(x_all, wg[q])) * dot(x_all, wu[q])).astype(BF))
        total = dot(hidden[0], wd[0]) + dot(hidden[1], wd[1])
        acc[g] = total[:rows]
        psend[g] = total[rows:].astype(BF)
        partial_copy(g).start()

    def finish(g):
        partial_copy(g).wait_recv()
        for s in range(SUB):
            cols = pl.ds(s * LANES, LANES)
            whole = acc[g, :, cols] + precv[g, :, cols].astype(F32)
            stage[pl.ds(s, rows, stride=SUB), :] = whole
        rsend[g] = stage[pl.ds(0, rows * SUB), :].astype(BF).reshape(per, cap, SUB, LANES)

        @pl.when(g == home)
        def _():
            ret[my_e] = rsend[home, core]

        dd = core + g // ny * (3 - 2 * core)
        t = (my_j + dd) % NX
        to_y = (y - g - 1 + chunks + ny) % ny
        for dz in range(nz):
            to_z = (z - dz + nz) % nz
            for c in range(CORES):

                def start():
                    pltpu.make_async_remote_copy(
                        src_ref=rsend.at[g, dz * CORES + c],
                        dst_ref=ret.at[my_e],
                        send_sem=r_send,
                        recv_sem=r_recv,
                        device_id=(place(to_z, to_y, c), t),
                        device_id_type=MESH,
                    ).start()

                if dz == 0:
                    pl.when(jnp.logical_or(g != home, core != c))(start)
                else:
                    start()

    for s in range(2):
        for a in range(6):
            src, dst = weight_piece(0, a, s)
            pltpu.make_async_copy(src, dst, w_recv.at[s, a]).wait()

    def step(i, carry):
        @pl.when(i < chunks)
        def _():
            arrive(i)

        @pl.when(jnp.logical_and(i >= LAG, i < chunks + LAG))
        def _():
            compute(i - LAG)

        @pl.when(i >= END_LAG)
        def _():
            finish(i - END_LAG)

        return carry

    lax.fori_loop(0, chunks + END_LAG, step, 0)

    got = ret.at[pl.ds(0, experts - 1)]
    pltpu.make_async_copy(got, got, r_recv).wait()

    for r in range(cap):
        stage[...] = ret[:, r].reshape(experts * SUB, LANES).astype(F32)
        for s in range(SUB):
            xbuf[pl.ds(r * experts, experts), pl.ds(s * LANES, LANES)] = stage[
                pl.ds(s, experts, stride=SUB), :
            ].astype(BF)
    mixed = dot(combine_w[...], xbuf[...])
    out[...] = (resid[...].astype(F32) + (mixed[:block] + mixed[block:])).astype(BF)

    sent = outg.at[pl.ds(0, experts - 1)]
    pltpu.make_async_copy(sent, sent, a_send).wait()
    pltpu.make_async_copy(got, got, r_send).wait()
    left = conv.at[pl.ds(0, NX - 1)]
    pltpu.make_async_copy(left, left, c_send).wait()
    for g in range(chunks):
        forward(g).wait_send()
        partial_copy(g).wait_send()

    @pl.when(sp < count - 1)
    def _():
        for a in range(3):
            edge_copy(a).wait_send()

    for l in range(2):
        d, slot, to = weight_plan(l)

        @pl.when(d != core)
        def _():
            for a in range(6):
                weight_copy(l, a, slot, to).wait_send()


def rows_of(conv):
    return conv.shape[1]


def body(
    ny,
    nz,
    stream,
    conv_value,
    conv_gate,
    doc_ids,
    conv_taps,
    conv_bias,
    chan_gain,
    chan_shift,
    out_weight,
    rms_gain,
    expert_ids,
    group_prob,
    route_logits,
    expert_gate,
    expert_up,
    expert_down,
):
    cap = 3
    tokens, width = stream.shape
    chunks = 2 * ny
    per = nz * CORES
    rows = per * cap
    experts = ny * nz * NX
    quarter = expert_gate.shape[2]
    channels = NX * LANES
    vmem = pl.BlockSpec(memory_space=pltpu.VMEM)
    hbm = pl.BlockSpec(memory_space=pl.ANY)
    dma = pltpu.SemaphoreType.DMA
    return pl.pallas_call(
        functools.partial(layer_kernel, ny, nz, cap),
        out_shape=jax.ShapeDtypeStruct((tokens, width), BF),
        in_specs=[hbm] + [vmem] * 7 + [hbm] + [vmem] * 4 + [hbm] * 3,
        out_specs=vmem,
        scratch_shapes=[
            pltpu.VMEM((HALO, LANES), BF),
            pltpu.VMEM((HALO, LANES), BF),
            pltpu.VMEM((NX, LANES), jnp.int32),
            pltpu.VMEM((HALO + NX * tokens, LANES), F32),
            pltpu.VMEM((HALO + NX * tokens, LANES), F32),
            pltpu.VMEM((NX, tokens, LANES), BF),
            pltpu.VMEM((NX, tokens, LANES), BF),
            pltpu.VMEM((tokens, channels), BF),
            pltpu.VMEM((tokens, width), BF),
            pltpu.VMEM((channels, width), BF),
            pltpu.VMEM((tokens, width), BF),
            pltpu.VMEM((experts * SUB, LANES), F32),
            pltpu.VMEM((experts * cap, width), BF),
            pltpu.VMEM((2 * tokens, experts * cap), BF),
            pltpu.VMEM((experts, cap, SUB, LANES), BF),
            pltpu.VMEM((chunks, per, cap, SUB, LANES), BF),
            pltpu.VMEM((chunks, per, cap, SUB, LANES), BF),
            pltpu.VMEM((2, width, quarter), BF),
            pltpu.VMEM((2, width, quarter), BF),
            pltpu.VMEM((2, quarter, width), BF),
            pltpu.VMEM((chunks, rows, width), F32),
            pltpu.VMEM((chunks, rows, width), BF),
            pltpu.VMEM((chunks, rows, width), BF),
            pltpu.VMEM((chunks, per, cap, SUB, LANES), BF),
            pltpu.VMEM((experts, cap, SUB, LANES), BF),
            pltpu.SemaphoreType.REGULAR,
            pltpu.SemaphoreType.REGULAR,
            dma((2,)),
            dma((3,)),
            dma((3,)),
            dma,
            dma,
            dma((2, 6)),
            dma((2, 6)),
            dma,
            dma((chunks,)),
            dma((chunks,)),
            dma((chunks,)),
            dma((chunks,)),
            dma((chunks,)),
            dma,
            dma,
        ],
        compiler_params=pltpu.CompilerParams(
            collective_id=0, has_side_effects=True, vmem_limit_bytes=60000 * 1024
        ),
    )(
        stream,
        conv_value,
        conv_gate,
        doc_ids.reshape(NX, LANES),
        conv_taps,
        conv_bias.reshape(1, LANES),
        chan_gain.reshape(1, channels),
        chan_shift.reshape(1, channels),
        out_weight,
        rms_gain.reshape(1, width),
        expert_ids,
        group_prob.reshape(1, LANES),
        route_logits,
        expert_gate,
        expert_up,
        expert_down,
    )


def solution(mesh):
    placed = (
        P(("sp", "tp"), None),
        P("sp", "tp"),
        P("sp", "tp"),
        P("sp"),
        P(None, "tp"),
        P("tp"),
        P(),
        P(),
        P(),
        P(),
        P(("sp", "tp"), None),
        P(("sp", "tp")),
        P(("sp", "tp"), None),
        P("sp", None, "tp"),
        P("sp", None, "tp"),
        P("sp", "tp", None),
    )
    ny = 4
    nz = mesh.shape["sp"] // (ny * CORES)
    return jax.shard_map(
        functools.partial(body, ny, nz),
        mesh=mesh,
        in_specs=placed,
        out_specs=P(("sp", "tp"), None),
        check_vma=False,
    )
```

```python
import functools

import jax
import jax.numpy as jnp
from jax import lax
from jax.experimental import pallas as pl
from jax.experimental.pallas import tpu as pltpu
from jax.sharding import PartitionSpec as P

eps = 1e-06
MESH = pl.DeviceIdType.MESH
NX = 4
CORES = 2
SUB = 16
LANES = 128
HALO = 32
LAG = 1
END_LAG = 2
F32 = jnp.float32
BF = jnp.bfloat16


def silu(v):
    return v / (1.0 + jnp.exp(-v))


def dot(a, b):
    return jnp.dot(a, b, preferred_element_type=F32)


def layer_kernel(
    ny,
    nz,
    cap,
    stream,
    value,
    gatein,
    docs,
    taps,
    bias,
    gain,
    shift,
    out_weight,
    rms_gain,
    ids,
    prob,
    logits,
    gate,
    up,
    down,
    out,
    halo_v,
    halo_g,
    halo_d,
    acts,
    docsb,
    conv,
    regroup,
    actv,
    stream_v,
    ow_v,
    resid,
    stage,
    xbuf,
    combine_w,
    outg,
    own,
    par,
    wg,
    wu,
    wd,
    acc,
    psend,
    precv,
    rsend,
    ret,
    near_sem,
    y_sem,
    reach_sem,
    z_sem,
    l_sem,
    h_send,
    h_recv,
    c_send,
    c_recv,
    w_send,
    w_recv,
    a_send,
    a_recv,
    f_send,
    f_recv,
    p_send,
    p_recv,
    r_send,
    r_recv,
):
    sp = lax.axis_index("sp")
    x = lax.axis_index("tp")
    core = sp % CORES
    ring = sp // CORES
    y = ring % ny
    z = ring // ny
    chunks = 2 * ny
    per = nz * CORES
    rows = per * cap
    experts = ny * nz * NX
    count = ny * nz * CORES
    block = rows_of(conv)
    reach = taps.shape[0] - 1
    width = resid.shape[1]

    def place(zz, yy, cc):
        return (zz * ny + yy) * CORES + cc

    def tell(sem, to):
        pl.semaphore_signal(sem, inc=1, device_id=to, device_id_type=MESH)

    def along_y(sem, steps):
        for dy in steps:
            tell(sem, (place(z, (y + dy) % ny, core), x))

    def along_z(sem, steps):
        for dz in steps:
            tell(sem, (place((z + dz) % nz, y, core), x))

    barrier = pltpu.get_barrier_semaphore()
    along_z(barrier, (1, nz - 1))
    along_y(barrier, (1, ny - 1))
    for dx in range(NX):
        for dc in range(CORES):
            if dx or dc:
                tell(barrier, (ring * CORES + (core + dc) % CORES, (x + dx) % NX))

    @pl.when(sp > 0)
    def _():
        tell(barrier, (sp - 1, x))

    load_ow = pltpu.make_async_copy(out_weight, ow_v, l_sem.at[0])
    load_stream = pltpu.make_async_copy(stream, stream_v, l_sem.at[1])
    load_ow.start()
    load_stream.start()

    tail = value.shape[0] - HALO
    edges = (
        (value.at[pl.ds(tail, HALO)], halo_v),
        (gatein.at[pl.ds(tail, HALO)], halo_g),
        (docs, halo_d),
    )

    def edge_copy(a):
        return pltpu.make_async_remote_copy(
            src_ref=edges[a][0],
            dst_ref=edges[a][1],
            send_sem=h_send.at[a],
            recv_sem=h_recv.at[a],
            device_id=(sp + 1, x),
            device_id_type=MESH,
        )

    triples = ((gate, wg), (up, wu), (down, wd))

    def weight_plan(l):
        j = CORES * core + l
        d = (x - j + NX) % NX
        slot = d // 2
        to_core = ((d + 1) // 2) % 2
        return d, slot, (ring * CORES + to_core, (j + to_core) % NX)

    def weight_piece(l, a, slot):
        src, dst = triples[a // 2]
        half = src.shape[1] // 2
        part = pl.ds(a % 2 * half, half)
        return src.at[l, part], dst.at[slot, part]

    def weight_copy(l, a, slot, to):
        src, dst = weight_piece(l, a, slot)
        return pltpu.make_async_remote_copy(
            src_ref=src,
            dst_ref=dst,
            send_sem=w_send.at[l, a],
            recv_sem=w_recv.at[slot, a],
            device_id=to,
            device_id_type=MESH,
        )

    def start_weights(kinds):
        for a in kinds:
            for l in range(2):
                d, slot, to = weight_plan(l)

                @pl.when(d == core)
                def _():
                    src, dst = weight_piece(l, a, slot)
                    pltpu.make_async_copy(src, dst, w_recv.at[slot, a]).start()

                @pl.when(d != core)
                def _():
                    weight_copy(l, a, slot, to).start()

    line = lax.broadcasted_iota(jnp.int32, (LANES, LANES), 0)
    lane = lax.broadcasted_iota(jnp.int32, (LANES, LANES), 1)
    ones = jnp.ones((LANES, LANES), BF)

    def spread(row):
        return dot(jnp.where(line == lane, row.astype(F32), 0.0).astype(BF), ones)

    def gated(v, g):
        return v.astype(F32) / (1.0 + jnp.exp(-g.astype(F32)))

    acts[pl.ds(HALO, NX * block), :] = gated(value[...], gatein[...])
    for b in range(NX):
        docsb[pl.ds(HALO + b * block, block), :] = spread(docs[pl.ds(b, 1), :])

    def conv_block(b):
        half = block // 2
        for piece in range(2):
            at = HALO + b * block + piece * half
            mine = docsb[pl.ds(at, half), :]
            total = jnp.broadcast_to(bias[...], (half, LANES))
            for j in range(reach + 1):
                same = docsb[pl.ds(at - j, half), :] == mine
                total = total + jnp.where(same, acts[pl.ds(at - j, half), :], 0.0) * taps[
                    pl.ds(j, 1), :
                ]
            conv[b, pl.ds(piece * half, half), :] = total.astype(BF)

    def hand_over(b):
        @pl.when(x == b)
        def _():
            regroup[b] = conv[b]

        @pl.when(x != b)
        def _():
            pltpu.make_async_remote_copy(
                src_ref=conv.at[b],
                dst_ref=regroup.at[x],
                send_sem=c_send,
                recv_sem=c_recv,
                device_id=(sp, b),
                device_id_type=MESH,
            ).start()

    for b in range(1, NX):
        conv_block(b)

    peers = NX * CORES - 1 + 4

    @pl.when(sp < count - 1)
    def _():
        pl.semaphore_wait(barrier, peers + 1)

    @pl.when(sp == count - 1)
    def _():
        pl.semaphore_wait(barrier, peers)

    along_z(near_sem, (1, nz - 1))
    along_y(near_sem, (1, ny - 1))

    @pl.when(sp < count - 1)
    def _():
        for a in range(3):
            edge_copy(a).start()

    for b in range(1, NX):
        hand_over(b)
    start_weights((0,))
    pl.semaphore_wait(near_sem, 4)
    along_y(y_sem, range(1, ny))
    along_z(reach_sem, (1, 2, nz - 2, nz - 1))

    @pl.when(sp == 0)
    def _():
        acts[pl.ds(0, HALO), :] = jnp.zeros((HALO, LANES), F32)
        docsb[pl.ds(0, HALO), :] = jnp.full((HALO, LANES), -1.0, F32)

    @pl.when(sp > 0)
    def _():
        for a in range(3):
            edge_copy(a).wait_recv()
        acts[pl.ds(0, HALO), :] = gated(halo_v[...], halo_g[...])
        docsb[pl.ds(0, HALO), :] = spread(halo_d[pl.ds(NX - 1, 1), :])[LANES - HALO :]

    conv_block(0)
    hand_over(0)
    start_weights(range(1, 6))
    pl.semaphore_wait(y_sem, ny - 1)
    pl.semaphore_wait(reach_sem, 4)
    along_z(z_sem, range(1, nz))

    first = ids[:, 0:1] == lane
    second = ids[:, 1:2] == lane
    match = jnp.where(jnp.logical_or(first, second), 1.0, 0.0)
    rank = dot(jnp.where(lane < line, 1.0, 0.0).astype(BF), match.astype(BF))
    share = jnp.sum(jnp.where(line == lane, prob[...], 0.0), axis=1, keepdims=True)
    gap = logits[:, 0:1] - logits[:, 1:2]
    w_first = share / (1.0 + jnp.exp(-gap))
    w_second = share / (1.0 + jnp.exp(gap))
    w_match = jnp.where(first, w_first, 0.0) + jnp.where(second, w_second, 0.0)
    picks = []
    for r in range(cap):
        at_rank = jnp.where(rank == float(r), match, 0.0)
        picks.append(at_rank.astype(BF))
        weight = at_rank * w_match
        high = weight.astype(BF)
        combine_w[pl.ds(0, block), pl.ds(r * LANES, LANES)] = high
        combine_w[pl.ds(block, block), pl.ds(r * LANES, LANES)] = (
            weight - high.astype(F32)
        ).astype(BF)

    pltpu.make_async_copy(
        regroup.at[pl.ds(0, NX - 1)], regroup.at[pl.ds(0, NX - 1)], c_recv
    ).wait()
    channels = NX * LANES
    parts = [regroup[b].astype(F32) for b in range(NX)]
    mean = jnp.sum(sum(parts[1:], parts[0]), axis=1, keepdims=True) / channels
    squares = [v * v for v in parts]
    square = jnp.sum(sum(squares[1:], squares[0]), axis=1, keepdims=True) / channels
    scale = lax.rsqrt(square - mean * mean + eps)
    for b in range(NX):
        cols = pl.ds(b * LANES, LANES)
        actv[:, cols] = silu((parts[b] - mean) * scale * gain[:, cols] + shift[:, cols]).astype(BF)
    load_ow.wait()
    load_stream.wait()
    summed = (stream_v[...].astype(F32) + dot(actv[...], ow_v[...])).astype(BF)
    resid[...] = summed
    wide = summed.astype(F32)
    power = jnp.sum(wide * wide, axis=1, keepdims=True) / width
    normed = (wide * lax.rsqrt(power + eps) * rms_gain[...]).astype(BF)

    for r in range(cap):
        rows_r = lax.dot_general(
            picks[r], normed, (((0,), (0,)), ((), ())), preferred_element_type=F32
        )
        for s in range(SUB):
            stage[pl.ds(s, experts, stride=SUB), :] = rows_r[:, s * LANES : (s + 1) * LANES]
        outg[:, r] = stage[...].astype(BF).reshape(experts, SUB, LANES)

    my_j = (x - core + NX) % NX
    my_e = ring * NX + my_j

    home = ny - 1
    own[home, core] = outg[my_e]

    def send_rows(g, carry):
        p = g // ny
        to_y = (y + g + 1) % ny
        for dz in spread_out(nz):
            base = ((z + dz) % nz) * ny + to_y
            for k in range(2):
                dd = 2 * p + (core + k) % 2
                j = (x - dd + NX) % NX
                m = ((dd + 1) // 2) % 2

                def start():
                    pltpu.make_async_remote_copy(
                        src_ref=outg.at[base * NX + j],
                        dst_ref=own.at[g, dz * CORES + core],
                        send_sem=a_send,
                        recv_sem=a_recv.at[g],
                        device_id=(base * CORES + m, (j + m) % NX),
                        device_id_type=MESH,
                    ).start()

                if dz == 0 and k == 0:
                    pl.when(g != home)(start)
                else:
                    start()
        return carry

    pl.semaphore_wait(z_sem, nz - 1)
    lax.fori_loop(0, chunks, send_rows, 0)

    mate = (ring * CORES + 1 - core, (x + 1 - 2 * core + NX) % NX)

    def forward(g):
        return pltpu.make_async_remote_copy(
            src_ref=own.at[g],
            dst_ref=par.at[g],
            send_sem=f_send.at[g],
            recv_sem=f_recv.at[g],
            device_id=mate,
            device_id_type=MESH,
        )

    def partial_copy(g):
        return pltpu.make_async_remote_copy(
            src_ref=psend.at[g],
            dst_ref=precv.at[g],
            send_sem=p_send.at[g],
            recv_sem=p_recv.at[g],
            device_id=mate,
            device_id_type=MESH,
        )

    def arrive(g):
        @pl.when(g == home)
        def _():
            part = own.at[home, pl.ds(0, per - 1)]
            pltpu.make_async_copy(part, part, a_recv.at[home]).wait()

        @pl.when(g != home)
        def _():
            pltpu.make_async_copy(own.at[g], own.at[g], a_recv.at[g]).wait()

        forward(g).start()

    def load_rows(buf, g, base):
        stage[pl.ds(0, rows * SUB), :] = buf[g].reshape(rows * SUB, LANES).astype(F32)
        for s in range(SUB):
            piece = stage[pl.ds(s, rows, stride=SUB), :]
            xbuf[pl.ds(base, rows), pl.ds(s * LANES, LANES)] = piece.astype(BF)

    def compute(g):
        load_rows(own, g, 0)
        forward(g).wait_recv()
        load_rows(par, g, rows)
        x_all = xbuf[pl.ds(0, 2 * rows), :]
        hidden = []
        for q in range(2):
            hidden.append((silu(dot(x_all, wg[q])) * dot(x_all, wu[q])).astype(BF))
        total = dot(hidden[0], wd[0]) + dot(hidden[1], wd[1])
        acc[g] = total[:rows]
        psend[g] = total[rows:].astype(BF)
        partial_copy(g).start()

    def finish(g):
        partial_copy(g).wait_recv()
        for s in range(SUB):
            cols = pl.ds(s * LANES, LANES)
            whole = acc[g, :, cols] + precv[g, :, cols].astype(F32)
            stage[pl.ds(s, rows, stride=SUB), :] = whole
        rsend[g] = stage[pl.ds(0, rows * SUB), :].astype(BF).reshape(per, cap, SUB, LANES)

        @pl.when(g == home)
        def _():
            ret[my_e] = rsend[home, core]

        dd = core + g // ny * (3 - 2 * core)
        t = (my_j + dd) % NX
        to_y = (y - g - 1 + chunks + ny) % ny
        for dz in spread_out(nz):
            to_z = (z - dz + nz) % nz
            for c in range(CORES):

                def start():
                    pltpu.make_async_remote_copy(
                        src_ref=rsend.at[g, dz * CORES + c],
                        dst_ref=ret.at[my_e],
                        send_sem=r_send,
                        recv_sem=r_recv,
                        device_id=(place(to_z, to_y, c), t),
                        device_id_type=MESH,
                    ).start()

                if dz == 0:
                    pl.when(jnp.logical_or(g != home, core != c))(start)
                else:
                    start()

    arrive(0)
    for s in range(2):
        for a in range(6):
            src, dst = weight_piece(0, a, s)
            pltpu.make_async_copy(src, dst, w_recv.at[s, a]).wait()

    def turn(i):
        q = i // 2
        return (q + (q + 1) // 2) % ny * 2 + i % 2

    def step(i, carry):
        @pl.when(jnp.logical_and(i > 0, i < chunks))
        def _():
            arrive(turn(i))

        @pl.when(jnp.logical_and(i >= LAG, i < chunks + LAG))
        def _():
            compute(turn(i - LAG))

        @pl.when(i >= END_LAG)
        def _():
            finish(turn(i - END_LAG))

        return carry

    lax.fori_loop(0, chunks + END_LAG, step, 0)

    got = ret.at[pl.ds(0, experts - 1)]
    pltpu.make_async_copy(got, got, r_recv).wait()

    for r in range(cap):
        stage[...] = ret[:, r].reshape(experts * SUB, LANES).astype(F32)
        for s in range(SUB):
            xbuf[pl.ds(r * experts, experts), pl.ds(s * LANES, LANES)] = stage[
                pl.ds(s, experts, stride=SUB), :
            ].astype(BF)
    mixed = dot(combine_w[...], xbuf[...])
    out[...] = (resid[...].astype(F32) + (mixed[:block] + mixed[block:])).astype(BF)

    sent = outg.at[pl.ds(0, experts - 1)]
    pltpu.make_async_copy(sent, sent, a_send).wait()
    pltpu.make_async_copy(got, got, r_send).wait()
    left = conv.at[pl.ds(0, NX - 1)]
    pltpu.make_async_copy(left, left, c_send).wait()
    for g in range(chunks):
        forward(g).wait_send()
        partial_copy(g).wait_send()

    @pl.when(sp < count - 1)
    def _():
        for a in range(3):
            edge_copy(a).wait_send()

    for l in range(2):
        d, slot, to = weight_plan(l)

        @pl.when(d != core)
        def _():
            for a in range(6):
                weight_copy(l, a, slot, to).wait_send()


def spread_out(size):
    return sorted(range(size), key=lambda d: (-min(d, size - d), d))


def rows_of(conv):
    return conv.shape[1]


def body(
    ny,
    nz,
    stream,
    conv_value,
    conv_gate,
    doc_ids,
    conv_taps,
    conv_bias,
    chan_gain,
    chan_shift,
    out_weight,
    rms_gain,
    expert_ids,
    group_prob,
    route_logits,
    expert_gate,
    expert_up,
    expert_down,
):
    cap = 3
    tokens, width = stream.shape
    chunks = 2 * ny
    per = nz * CORES
    rows = per * cap
    experts = ny * nz * NX
    quarter = expert_gate.shape[2]
    channels = NX * LANES
    vmem = pl.BlockSpec(memory_space=pltpu.VMEM)
    hbm = pl.BlockSpec(memory_space=pl.ANY)
    dma = pltpu.SemaphoreType.DMA
    return pl.pallas_call(
        functools.partial(layer_kernel, ny, nz, cap),
        out_shape=jax.ShapeDtypeStruct((tokens, width), BF),
        in_specs=[hbm] + [vmem] * 7 + [hbm] + [vmem] * 4 + [hbm] * 3,
        out_specs=vmem,
        scratch_shapes=[
            pltpu.VMEM((HALO, LANES), BF),
            pltpu.VMEM((HALO, LANES), BF),
            pltpu.VMEM((NX, LANES), jnp.int32),
            pltpu.VMEM((HALO + NX * tokens, LANES), F32),
            pltpu.VMEM((HALO + NX * tokens, LANES), F32),
            pltpu.VMEM((NX, tokens, LANES), BF),
            pltpu.VMEM((NX, tokens, LANES), BF),
            pltpu.VMEM((tokens, channels), BF),
            pltpu.VMEM((tokens, width), BF),
            pltpu.VMEM((channels, width), BF),
            pltpu.VMEM((tokens, width), BF),
            pltpu.VMEM((experts * SUB, LANES), F32),
            pltpu.VMEM((experts * cap, width), BF),
            pltpu.VMEM((2 * tokens, experts * cap), BF),
            pltpu.VMEM((experts, cap, SUB, LANES), BF),
            pltpu.VMEM((chunks, per, cap, SUB, LANES), BF),
            pltpu.VMEM((chunks, per, cap, SUB, LANES), BF),
            pltpu.VMEM((2, width, quarter), BF),
            pltpu.VMEM((2, width, quarter), BF),
            pltpu.VMEM((2, quarter, width), BF),
            pltpu.VMEM((chunks, rows, width), F32),
            pltpu.VMEM((chunks, rows, width), BF),
            pltpu.VMEM((chunks, rows, width), BF),
            pltpu.VMEM((chunks, per, cap, SUB, LANES), BF),
            pltpu.VMEM((experts, cap, SUB, LANES), BF),
            pltpu.SemaphoreType.REGULAR,
            pltpu.SemaphoreType.REGULAR,
            pltpu.SemaphoreType.REGULAR,
            pltpu.SemaphoreType.REGULAR,
            dma((2,)),
            dma((3,)),
            dma((3,)),
            dma,
            dma,
            dma((2, 6)),
            dma((2, 6)),
            dma,
            dma((chunks,)),
            dma((chunks,)),
            dma((chunks,)),
            dma((chunks,)),
            dma((chunks,)),
            dma,
            dma,
        ],
        compiler_params=pltpu.CompilerParams(
            collective_id=0, has_side_effects=True, vmem_limit_bytes=60000 * 1024
        ),
    )(
        stream,
        conv_value,
        conv_gate,
        doc_ids.reshape(NX, LANES),
        conv_taps,
        conv_bias.reshape(1, LANES),
        chan_gain.reshape(1, channels),
        chan_shift.reshape(1, channels),
        out_weight,
        rms_gain.reshape(1, width),
        expert_ids,
        group_prob.reshape(1, LANES),
        route_logits,
        expert_gate,
        expert_up,
        expert_down,
    )


def solution(mesh):
    placed = (
        P(("sp", "tp"), None),
        P("sp", "tp"),
        P("sp", "tp"),
        P("sp"),
        P(None, "tp"),
        P("tp"),
        P(),
        P(),
        P(),
        P(),
        P(("sp", "tp"), None),
        P(("sp", "tp")),
        P(("sp", "tp"), None),
        P("sp", None, "tp"),
        P("sp", None, "tp"),
        P("sp", "tp", None),
    )
    ny = 4
    nz = mesh.shape["sp"] // (ny * CORES)
    return jax.shard_map(
        functools.partial(body, ny, nz),
        mesh=mesh,
        in_specs=placed,
        out_specs=P(("sp", "tp"), None),
        check_vma=False,
    )
```

```python
import functools

import jax
import jax.numpy as jnp
from jax import lax
from jax.experimental import pallas as pl
from jax.experimental.pallas import tpu as pltpu
from jax.sharding import PartitionSpec as P

eps = 1e-06
MESH = pl.DeviceIdType.MESH
NX = 4
CORES = 2
SUB = 16
LANES = 128
HALO = 32
LAG = 1
END_LAG = 2
F32 = jnp.float32
BF = jnp.bfloat16


def silu(v):
    return v / (1.0 + jnp.exp(-v))


def dot(a, b):
    return jnp.dot(a, b, preferred_element_type=F32)


def layer_kernel(
    ny,
    nz,
    cap,
    stream,
    value_in,
    gatein_in,
    docs_in,
    taps_in,
    bias_in,
    gain_in,
    shift_in,
    out_weight,
    rms_gain_in,
    ids_in,
    prob_in,
    logits_in,
    gate,
    up,
    down,
    out,
    value,
    gatein,
    docs,
    taps,
    bias,
    gain,
    shift,
    rms_gain,
    ids,
    prob,
    logits,
    halo_v,
    halo_g,
    halo_d,
    acts,
    docsb,
    conv,
    regroup,
    actv,
    stream_v,
    ow_v,
    resid,
    stage,
    xbuf,
    combine_w,
    outg,
    own,
    par,
    wg,
    wu,
    wd,
    acc,
    psend,
    precv,
    rsend,
    ret,
    o_sem,
    near_sem,
    y_sem,
    reach_sem,
    z_sem,
    l_sem,
    h_send,
    h_recv,
    c_send,
    c_recv,
    w_send,
    w_recv,
    a_send,
    a_recv,
    f_send,
    f_recv,
    p_send,
    p_recv,
    r_send,
    r_recv,
):
    sp = lax.axis_index("sp")
    x = lax.axis_index("tp")
    core = sp % CORES
    ring = sp // CORES
    y = ring % ny
    z = ring // ny
    chunks = 2 * ny
    per = nz * CORES
    member = (core + (x + 1) // 2) % CORES

    def seat(m, at_x):
        return (m + (at_x + 1) // 2) % CORES

    rows = per * cap
    experts = ny * nz * NX
    count = ny * nz * CORES
    block = rows_of(conv)
    reach = taps.shape[0] - 1
    width = resid.shape[1]

    def place(zz, yy, cc):
        return (zz * ny + yy) * CORES + cc

    def tell(sem, to):
        pl.semaphore_signal(sem, inc=1, device_id=to, device_id_type=MESH)

    def along_y(sem, steps):
        for dy in steps:
            tell(sem, (place(z, (y + dy) % ny, core), x))

    def along_z(sem, steps):
        for dz in steps:
            tell(sem, (place((z + dz) % nz, y, core), x))

    barrier = pltpu.get_barrier_semaphore()
    along_z(barrier, (1, nz - 1))
    along_y(barrier, (1, ny - 1))
    for dx in range(NX):
        for dc in range(CORES):
            if dx or dc:
                tell(barrier, (ring * CORES + (core + dc) % CORES, (x + dx) % NX))

    @pl.when(sp > 0)
    def _():
        tell(barrier, (sp - 1, x))

    small = (
        (value_in, value),
        (gatein_in, gatein),
        (docs_in, docs),
        (taps_in, taps),
        (bias_in, bias),
        (gain_in, gain),
        (shift_in, shift),
        (rms_gain_in, rms_gain),
        (ids_in, ids),
        (prob_in, prob),
        (logits_in, logits),
    )
    loads = [pltpu.make_async_copy(a, b, o_sem.at[i]) for i, (a, b) in enumerate(small)]
    for load in loads:
        load.start()
    load_ow = pltpu.make_async_copy(out_weight, ow_v, l_sem.at[0])
    load_stream = pltpu.make_async_copy(stream, stream_v, l_sem.at[1])
    load_ow.start()
    load_stream.start()

    tail = value.shape[0] - HALO
    edges = (
        (value.at[pl.ds(tail, HALO)], halo_v),
        (gatein.at[pl.ds(tail, HALO)], halo_g),
        (docs, halo_d),
    )

    def edge_copy(a):
        return pltpu.make_async_remote_copy(
            src_ref=edges[a][0],
            dst_ref=edges[a][1],
            send_sem=h_send.at[a],
            recv_sem=h_recv.at[a],
            device_id=(sp + 1, x),
            device_id_type=MESH,
        )

    triples = ((gate, wg), (up, wu), (down, wd))

    def weight_plan(l):
        j = CORES * core + l
        d = (x - j + NX) % NX
        slot = d // 2
        m = ((d + 1) // 2) % 2
        to_x = (j + m) % NX
        return d, slot, (ring * CORES + seat(m, to_x), to_x)

    def weight_piece(l, a, slot):
        src, dst = triples[a // 2]
        half = src.shape[1] // 2
        part = pl.ds(a % 2 * half, half)
        return src.at[l, part], dst.at[slot, part]

    def weight_copy(l, a, slot, to):
        src, dst = weight_piece(l, a, slot)
        return pltpu.make_async_remote_copy(
            src_ref=src,
            dst_ref=dst,
            send_sem=w_send.at[l, a],
            recv_sem=w_recv.at[slot, a],
            device_id=to,
            device_id_type=MESH,
        )

    def start_weights(kinds):
        for a in kinds:
            for l in range(2):
                d, slot, to = weight_plan(l)

                @pl.when(d == member)
                def _():
                    src, dst = weight_piece(l, a, slot)
                    pltpu.make_async_copy(src, dst, w_recv.at[slot, a]).start()

                @pl.when(d != member)
                def _():
                    weight_copy(l, a, slot, to).start()

    line = lax.broadcasted_iota(jnp.int32, (LANES, LANES), 0)
    lane = lax.broadcasted_iota(jnp.int32, (LANES, LANES), 1)
    ones = jnp.ones((LANES, LANES), BF)

    def spread(row):
        return dot(jnp.where(line == lane, row.astype(F32), 0.0).astype(BF), ones)

    def gated(v, g):
        return v.astype(F32) / (1.0 + jnp.exp(-g.astype(F32)))

    for load in loads:
        load.wait()
    acts[pl.ds(HALO, NX * block), :] = gated(value[...], gatein[...])
    for b in range(NX):
        docsb[pl.ds(HALO + b * block, block), :] = spread(docs[pl.ds(b, 1), :])

    def conv_block(b):
        half = block // 2
        for piece in range(2):
            at = HALO + b * block + piece * half
            mine = docsb[pl.ds(at, half), :]
            total = jnp.broadcast_to(bias[...], (half, LANES))
            for j in range(reach + 1):
                same = docsb[pl.ds(at - j, half), :] == mine
                total = total + jnp.where(same, acts[pl.ds(at - j, half), :], 0.0) * taps[
                    pl.ds(j, 1), :
                ]
            conv[b, pl.ds(piece * half, half), :] = total.astype(BF)

    def hand_over(b):
        @pl.when(x == b)
        def _():
            regroup[b] = conv[b]

        @pl.when(x != b)
        def _():
            pltpu.make_async_remote_copy(
                src_ref=conv.at[b],
                dst_ref=regroup.at[x],
                send_sem=c_send,
                recv_sem=c_recv,
                device_id=(sp, b),
                device_id_type=MESH,
            ).start()

    for b in range(1, NX):
        conv_block(b)

    peers = NX * CORES - 1 + 4

    @pl.when(sp < count - 1)
    def _():
        pl.semaphore_wait(barrier, peers + 1)

    @pl.when(sp == count - 1)
    def _():
        pl.semaphore_wait(barrier, peers)

    along_z(near_sem, (1, nz - 1))
    along_y(near_sem, (1, ny - 1))

    @pl.when(sp < count - 1)
    def _():
        for a in range(3):
            edge_copy(a).start()

    for b in range(1, NX):
        hand_over(b)
    start_weights((0,))
    pl.semaphore_wait(near_sem, 4)
    along_y(y_sem, range(1, ny))
    along_z(reach_sem, (1, 2, nz - 2, nz - 1))

    @pl.when(sp == 0)
    def _():
        acts[pl.ds(0, HALO), :] = jnp.zeros((HALO, LANES), F32)
        docsb[pl.ds(0, HALO), :] = jnp.full((HALO, LANES), -1.0, F32)

    @pl.when(sp > 0)
    def _():
        for a in range(3):
            edge_copy(a).wait_recv()
        acts[pl.ds(0, HALO), :] = gated(halo_v[...], halo_g[...])
        docsb[pl.ds(0, HALO), :] = spread(halo_d[pl.ds(NX - 1, 1), :])[LANES - HALO :]

    conv_block(0)
    hand_over(0)
    start_weights(range(1, 6))
    pl.semaphore_wait(y_sem, ny - 1)
    pl.semaphore_wait(reach_sem, 4)
    along_z(z_sem, range(1, nz))

    first = spread(ids[pl.ds(0, 1), :]) == lane.astype(F32)
    second = spread(ids[pl.ds(1, 1), :]) == lane.astype(F32)
    match = jnp.where(jnp.logical_or(first, second), 1.0, 0.0)
    rank = dot(jnp.where(lane < line, 1.0, 0.0).astype(BF), match.astype(BF))

    def column(row):
        return jnp.sum(jnp.where(line == lane, row, 0.0), axis=1, keepdims=True)

    gap = logits[pl.ds(0, 1), :] - logits[pl.ds(1, 1), :]
    w_first = column(prob[...] / (1.0 + jnp.exp(-gap)))
    w_second = column(prob[...] / (1.0 + jnp.exp(gap)))
    w_match = jnp.where(first, w_first, 0.0) + jnp.where(second, w_second, 0.0)
    picks = []
    for r in range(cap):
        at_rank = jnp.where(rank == float(r), match, 0.0)
        picks.append(at_rank.astype(BF))
        weight = at_rank * w_match
        high = weight.astype(BF)
        combine_w[pl.ds(0, block), pl.ds(r * LANES, LANES)] = high
        combine_w[pl.ds(block, block), pl.ds(r * LANES, LANES)] = (
            weight - high.astype(F32)
        ).astype(BF)

    pltpu.make_async_copy(
        regroup.at[pl.ds(0, NX - 1)], regroup.at[pl.ds(0, NX - 1)], c_recv
    ).wait()
    channels = NX * LANES
    parts = [regroup[b].astype(F32) for b in range(NX)]
    mean = jnp.sum(sum(parts[1:], parts[0]), axis=1, keepdims=True) / channels
    squares = [v * v for v in parts]
    square = jnp.sum(sum(squares[1:], squares[0]), axis=1, keepdims=True) / channels
    scale = lax.rsqrt(square - mean * mean + eps)
    for b in range(NX):
        cols = pl.ds(b * LANES, LANES)
        actv[:, cols] = silu((parts[b] - mean) * scale * gain[:, cols] + shift[:, cols]).astype(BF)
    load_ow.wait()
    load_stream.wait()
    summed = (stream_v[...].astype(F32) + dot(actv[...], ow_v[...])).astype(BF)
    resid[...] = summed
    wide = summed.astype(F32)
    power = jnp.sum(wide * wide, axis=1, keepdims=True) / width
    normed = (wide * lax.rsqrt(power + eps) * rms_gain[...]).astype(BF)

    for r in range(cap):
        rows_r = lax.dot_general(
            picks[r], normed, (((0,), (0,)), ((), ())), preferred_element_type=F32
        )
        for s in range(SUB):
            stage[pl.ds(s, experts, stride=SUB), :] = rows_r[:, s * LANES : (s + 1) * LANES]
        outg[:, r] = stage[...].astype(BF).reshape(experts, SUB, LANES)

    my_j = (x - member + NX) % NX
    my_e = ring * NX + my_j

    home = ny - 1
    own[home, core] = outg[my_e]

    def send_rows(g, carry):
        p = g // ny
        to_y = (y + g + 1) % ny
        for dz in spread_out(nz):
            base = ((z + dz) % nz) * ny + to_y
            for k in range(2):
                dd = 2 * p + (member + k) % 2
                j = (x - dd + NX) % NX
                m = ((dd + 1) // 2) % 2
                to_x = (j + m) % NX

                def start():
                    pltpu.make_async_remote_copy(
                        src_ref=outg.at[base * NX + j],
                        dst_ref=own.at[g, dz * CORES + core],
                        send_sem=a_send,
                        recv_sem=a_recv.at[g],
                        device_id=(base * CORES + seat(m, to_x), to_x),
                        device_id_type=MESH,
                    ).start()

                if dz == 0 and k == 0:
                    pl.when(g != home)(start)
                else:
                    start()
        return carry

    pl.semaphore_wait(z_sem, nz - 1)
    lax.fori_loop(0, chunks, send_rows, 0)

    mate_x = (x + 1 - 2 * member + NX) % NX
    mate = (ring * CORES + seat(1 - member, mate_x), mate_x)

    def forward(g):
        return pltpu.make_async_remote_copy(
            src_ref=own.at[g],
            dst_ref=par.at[g],
            send_sem=f_send.at[g],
            recv_sem=f_recv.at[g],
            device_id=mate,
            device_id_type=MESH,
        )

    def partial_copy(g):
        return pltpu.make_async_remote_copy(
            src_ref=psend.at[g],
            dst_ref=precv.at[g],
            send_sem=p_send.at[g],
            recv_sem=p_recv.at[g],
            device_id=mate,
            device_id_type=MESH,
        )

    def arrive(g):
        @pl.when(g == home)
        def _():
            part = own.at[home, pl.ds(0, per - 1)]
            pltpu.make_async_copy(part, part, a_recv.at[home]).wait()

        @pl.when(g != home)
        def _():
            pltpu.make_async_copy(own.at[g], own.at[g], a_recv.at[g]).wait()

        forward(g).start()

    def load_rows(buf, g, base):
        stage[pl.ds(0, rows * SUB), :] = buf[g].reshape(rows * SUB, LANES).astype(F32)
        for s in range(SUB):
            piece = stage[pl.ds(s, rows, stride=SUB), :]
            xbuf[pl.ds(base, rows), pl.ds(s * LANES, LANES)] = piece.astype(BF)

    def compute(g):
        load_rows(own, g, 0)
        forward(g).wait_recv()
        load_rows(par, g, rows)
        x_all = xbuf[pl.ds(0, 2 * rows), :]
        hidden = []
        for q in range(2):
            hidden.append((silu(dot(x_all, wg[q])) * dot(x_all, wu[q])).astype(BF))
        total = dot(hidden[0], wd[0]) + dot(hidden[1], wd[1])
        acc[g] = total[:rows]
        psend[g] = total[rows:].astype(BF)
        partial_copy(g).start()

    def finish(g):
        partial_copy(g).wait_recv()
        for s in range(SUB):
            cols = pl.ds(s * LANES, LANES)
            whole = acc[g, :, cols] + precv[g, :, cols].astype(F32)
            stage[pl.ds(s, rows, stride=SUB), :] = whole
        rsend[g] = stage[pl.ds(0, rows * SUB), :].astype(BF).reshape(per, cap, SUB, LANES)

        @pl.when(g == home)
        def _():
            ret[my_e] = rsend[home, core]

        dd = member + g // ny * (3 - 2 * member)
        t = (my_j + dd) % NX
        to_y = (y - g - 1 + chunks + ny) % ny
        for dz in spread_out(nz):
            to_z = (z - dz + nz) % nz
            for c in range(CORES):

                def start():
                    pltpu.make_async_remote_copy(
                        src_ref=rsend.at[g, dz * CORES + c],
                        dst_ref=ret.at[my_e],
                        send_sem=r_send,
                        recv_sem=r_recv,
                        device_id=(place(to_z, to_y, c), t),
                        device_id_type=MESH,
                    ).start()

                if dz == 0:
                    pl.when(jnp.logical_or(g != home, core != c))(start)
                else:
                    start()

    arrive(0)
    arrive(1)
    for s in range(2):
        for a in range(6):
            src, dst = weight_piece(0, a, s)
            pltpu.make_async_copy(src, dst, w_recv.at[s, a]).wait()

    def turn(i):
        q = i // 2
        return (q + (q + 1) // 2) % ny * 2 + i % 2

    def step(i, carry):
        @pl.when(jnp.logical_and(i > 1, i < chunks))
        def _():
            arrive(turn(i))

        @pl.when(jnp.logical_and(i >= LAG, i < chunks + LAG))
        def _():
            compute(turn(i - LAG))

        @pl.when(i >= END_LAG)
        def _():
            finish(turn(i - END_LAG))

        return carry

    lax.fori_loop(0, chunks + END_LAG, step, 0)

    got = ret.at[pl.ds(0, experts - 1)]
    pltpu.make_async_copy(got, got, r_recv).wait()

    for r in range(cap):
        stage[...] = ret[:, r].reshape(experts * SUB, LANES).astype(F32)
        for s in range(SUB):
            xbuf[pl.ds(r * experts, experts), pl.ds(s * LANES, LANES)] = stage[
                pl.ds(s, experts, stride=SUB), :
            ].astype(BF)
    mixed = dot(combine_w[...], xbuf[...])
    out[...] = (resid[...].astype(F32) + (mixed[:block] + mixed[block:])).astype(BF)

    sent = outg.at[pl.ds(0, experts - 1)]
    pltpu.make_async_copy(sent, sent, a_send).wait()
    pltpu.make_async_copy(got, got, r_send).wait()
    left = conv.at[pl.ds(0, NX - 1)]
    pltpu.make_async_copy(left, left, c_send).wait()
    for g in range(chunks):
        forward(g).wait_send()
        partial_copy(g).wait_send()

    @pl.when(sp < count - 1)
    def _():
        for a in range(3):
            edge_copy(a).wait_send()

    for l in range(2):
        d, slot, to = weight_plan(l)

        @pl.when(d != member)
        def _():
            for a in range(6):
                weight_copy(l, a, slot, to).wait_send()


def spread_out(size):
    return sorted(range(size), key=lambda d: (-min(d, size - d), d))


def rows_of(conv):
    return conv.shape[1]


def body(
    ny,
    nz,
    stream,
    conv_value,
    conv_gate,
    doc_ids,
    conv_taps,
    conv_bias,
    chan_gain,
    chan_shift,
    out_weight,
    rms_gain,
    expert_ids,
    group_prob,
    route_logits,
    expert_gate,
    expert_up,
    expert_down,
):
    cap = 3
    tokens, width = stream.shape
    chunks = 2 * ny
    per = nz * CORES
    rows = per * cap
    experts = ny * nz * NX
    quarter = expert_gate.shape[2]
    channels = NX * LANES
    vmem = pl.BlockSpec(memory_space=pltpu.VMEM)
    hbm = pl.BlockSpec(memory_space=pl.ANY)
    dma = pltpu.SemaphoreType.DMA
    return pl.pallas_call(
        functools.partial(layer_kernel, ny, nz, cap),
        out_shape=jax.ShapeDtypeStruct((tokens, width), BF),
        in_specs=[hbm] * 16,
        out_specs=vmem,
        scratch_shapes=[
            pltpu.VMEM((NX * tokens, LANES), BF),
            pltpu.VMEM((NX * tokens, LANES), BF),
            pltpu.VMEM((NX, LANES), jnp.int32),
            pltpu.VMEM(conv_taps.shape, F32),
            pltpu.VMEM((1, LANES), F32),
            pltpu.VMEM((1, channels), F32),
            pltpu.VMEM((1, channels), F32),
            pltpu.VMEM((1, width), F32),
            pltpu.VMEM((2, LANES), jnp.int32),
            pltpu.VMEM((1, LANES), F32),
            pltpu.VMEM((2, LANES), F32),
            pltpu.VMEM((HALO, LANES), BF),
            pltpu.VMEM((HALO, LANES), BF),
            pltpu.VMEM((NX, LANES), jnp.int32),
            pltpu.VMEM((HALO + NX * tokens, LANES), F32),
            pltpu.VMEM((HALO + NX * tokens, LANES), F32),
            pltpu.VMEM((NX, tokens, LANES), BF),
            pltpu.VMEM((NX, tokens, LANES), BF),
            pltpu.VMEM((tokens, channels), BF),
            pltpu.VMEM((tokens, width), BF),
            pltpu.VMEM((channels, width), BF),
            pltpu.VMEM((tokens, width), BF),
            pltpu.VMEM((experts * SUB, LANES), F32),
            pltpu.VMEM((experts * cap, width), BF),
            pltpu.VMEM((2 * tokens, experts * cap), BF),
            pltpu.VMEM((experts, cap, SUB, LANES), BF),
            pltpu.VMEM((chunks, per, cap, SUB, LANES), BF),
            pltpu.VMEM((chunks, per, cap, SUB, LANES), BF),
            pltpu.VMEM((2, width, quarter), BF),
            pltpu.VMEM((2, width, quarter), BF),
            pltpu.VMEM((2, quarter, width), BF),
            pltpu.VMEM((chunks, rows, width), F32),
            pltpu.VMEM((chunks, rows, width), BF),
            pltpu.VMEM((chunks, rows, width), BF),
            pltpu.VMEM((chunks, per, cap, SUB, LANES), BF),
            pltpu.VMEM((experts, cap, SUB, LANES), BF),
            dma((11,)),
            pltpu.SemaphoreType.REGULAR,
            pltpu.SemaphoreType.REGULAR,
            pltpu.SemaphoreType.REGULAR,
            pltpu.SemaphoreType.REGULAR,
            dma((2,)),
            dma((3,)),
            dma((3,)),
            dma,
            dma,
            dma((2, 6)),
            dma((2, 6)),
            dma,
            dma((chunks,)),
            dma((chunks,)),
            dma((chunks,)),
            dma((chunks,)),
            dma((chunks,)),
            dma,
            dma,
        ],
        compiler_params=pltpu.CompilerParams(
            collective_id=0, has_side_effects=True, vmem_limit_bytes=60000 * 1024
        ),
    )(
        stream,
        conv_value,
        conv_gate,
        doc_ids.reshape(NX, LANES),
        conv_taps,
        conv_bias.reshape(1, LANES),
        chan_gain.reshape(1, channels),
        chan_shift.reshape(1, channels),
        out_weight,
        rms_gain.reshape(1, width),
        expert_ids.T,
        group_prob.reshape(1, LANES),
        route_logits.T,
        expert_gate,
        expert_up,
        expert_down,
    )


def solution(mesh):
    placed = (
        P(("sp", "tp"), None),
        P("sp", "tp"),
        P("sp", "tp"),
        P("sp"),
        P(None, "tp"),
        P("tp"),
        P(),
        P(),
        P(),
        P(),
        P(("sp", "tp"), None),
        P(("sp", "tp")),
        P(("sp", "tp"), None),
        P("sp", None, "tp"),
        P("sp", None, "tp"),
        P("sp", "tp", None),
    )
    ny = 4
    nz = mesh.shape["sp"] // (ny * CORES)
    return jax.shard_map(
        functools.partial(body, ny, nz),
        mesh=mesh,
        in_specs=placed,
        out_specs=P(("sp", "tp"), None),
        check_vma=False,
    )
```

```python
import functools

import jax
import jax.numpy as jnp
from jax import lax
from jax.experimental import pallas as pl
from jax.experimental.pallas import tpu as pltpu
from jax.sharding import PartitionSpec as P

eps = 1e-06
MESH = pl.DeviceIdType.MESH
NX = 4
CORES = 2
SUB = 16
LANES = 128
HALO = 32
LAG = 1
END_LAG = 2
F32 = jnp.float32
BF = jnp.bfloat16


def silu(v):
    return v / (1.0 + jnp.exp(-v))


def dot(a, b):
    return jnp.dot(a, b, preferred_element_type=F32)


def layer_kernel(
    ny,
    nz,
    cap,
    stream,
    value_in,
    gatein_in,
    docs_in,
    taps_in,
    bias_in,
    gain_in,
    shift_in,
    out_weight,
    rms_gain_in,
    ids_in,
    prob_in,
    logits_in,
    gate,
    up,
    down,
    out,
    value,
    gatein,
    docs,
    taps,
    bias,
    gain,
    shift,
    rms_gain,
    ids,
    prob,
    logits,
    halo_v,
    halo_g,
    halo_d,
    acts,
    docsb,
    conv,
    regroup,
    actv,
    stream_v,
    ow_v,
    resid,
    stage,
    xbuf,
    combine_w,
    outg,
    own,
    par,
    wg,
    wu,
    wd,
    acc,
    psend,
    precv,
    rsend,
    ret,
    o_sem,
    near_sem,
    y_sem,
    reach_sem,
    z_sem,
    l_sem,
    h_send,
    h_recv,
    c_send,
    c_recv,
    w_send,
    w_recv,
    a_send,
    a_recv,
    f_send,
    f_recv,
    p_send,
    p_recv,
    r_send,
    r_recv,
):
    sp = lax.axis_index("sp")
    x = lax.axis_index("tp")
    core = sp % CORES
    ring = sp // CORES
    y = ring % ny
    z = ring // ny
    chunks = 2 * ny
    per = nz * CORES
    member = (core + (x + 1) // 2) % CORES

    def seat(m, at_x):
        return (m + (at_x + 1) // 2) % CORES

    rows = per * cap
    experts = ny * nz * NX
    count = ny * nz * CORES
    block = rows_of(conv)
    reach = taps.shape[0] - 1
    width = resid.shape[1]

    def place(zz, yy, cc):
        return (zz * ny + yy) * CORES + cc

    def tell(sem, to):
        pl.semaphore_signal(sem, inc=1, device_id=to, device_id_type=MESH)

    def along_y(sem, steps):
        for dy in steps:
            tell(sem, (place(z, (y + dy) % ny, core), x))

    def along_z(sem, steps):
        for dz in steps:
            tell(sem, (place((z + dz) % nz, y, core), x))

    barrier = pltpu.get_barrier_semaphore()
    along_z(barrier, (1, nz - 1))
    along_y(barrier, (1, ny - 1))
    for dx in range(NX):
        for dc in range(CORES):
            if dx or dc:
                tell(barrier, (ring * CORES + (core + dc) % CORES, (x + dx) % NX))

    @pl.when(sp > 0)
    def _():
        tell(barrier, (sp - 1, x))

    small = (
        (value_in, value),
        (gatein_in, gatein),
        (docs_in, docs),
        (taps_in, taps),
        (bias_in, bias),
        (gain_in, gain),
        (shift_in, shift),
        (rms_gain_in, rms_gain),
        (ids_in, ids),
        (prob_in, prob),
        (logits_in, logits),
    )
    loads = [pltpu.make_async_copy(a, b, o_sem.at[i]) for i, (a, b) in enumerate(small)]
    for load in loads:
        load.start()
    load_ow = pltpu.make_async_copy(out_weight, ow_v, l_sem.at[0])
    load_stream = pltpu.make_async_copy(stream, stream_v, l_sem.at[1])
    load_ow.start()
    load_stream.start()

    tail = value.shape[0] - HALO
    edges = (
        (value.at[pl.ds(tail, HALO)], halo_v),
        (gatein.at[pl.ds(tail, HALO)], halo_g),
        (docs, halo_d),
    )

    def edge_copy(a):
        return pltpu.make_async_remote_copy(
            src_ref=edges[a][0],
            dst_ref=edges[a][1],
            send_sem=h_send.at[a],
            recv_sem=h_recv.at[a],
            device_id=(sp + 1, x),
            device_id_type=MESH,
        )

    triples = ((gate, wg), (up, wu), (down, wd))

    def weight_plan(l):
        j = CORES * core + l
        d = (x - j + NX) % NX
        slot = d // 2
        m = ((d + 1) // 2) % 2
        to_x = (j + m) % NX
        return d, slot, (ring * CORES + seat(m, to_x), to_x)

    def weight_piece(l, a, slot):
        src, dst = triples[a // 2]
        half = src.shape[1] // 2
        part = pl.ds(a % 2 * half, half)
        return src.at[l, part], dst.at[slot, part]

    def weight_copy(l, a, slot, to):
        src, dst = weight_piece(l, a, slot)
        return pltpu.make_async_remote_copy(
            src_ref=src,
            dst_ref=dst,
            send_sem=w_send.at[l, a],
            recv_sem=w_recv.at[slot, a],
            device_id=to,
            device_id_type=MESH,
        )

    def start_weights(kinds):
        for a in kinds:
            for l in range(2):
                d, slot, to = weight_plan(l)

                @pl.when(d == member)
                def _():
                    src, dst = weight_piece(l, a, slot)
                    pltpu.make_async_copy(src, dst, w_recv.at[slot, a]).start()

                @pl.when(d != member)
                def _():
                    weight_copy(l, a, slot, to).start()

    line = lax.broadcasted_iota(jnp.int32, (LANES, LANES), 0)
    lane = lax.broadcasted_iota(jnp.int32, (LANES, LANES), 1)
    ones = jnp.ones((LANES, LANES), BF)

    def spread(row):
        return dot(jnp.where(line == lane, row.astype(F32), 0.0).astype(BF), ones)

    def gated(v, g):
        return v.astype(F32) / (1.0 + jnp.exp(-g.astype(F32)))

    for load in loads:
        load.wait()
    acts[pl.ds(HALO, NX * block), :] = gated(value[...], gatein[...])
    for b in range(NX):
        docsb[pl.ds(HALO + b * block, block), :] = spread(docs[pl.ds(b, 1), :])

    def conv_block(b):
        half = block // 2
        for piece in range(2):
            at = HALO + b * block + piece * half
            mine = docsb[pl.ds(at, half), :]
            total = jnp.broadcast_to(bias[...], (half, LANES))
            for j in range(reach + 1):
                same = docsb[pl.ds(at - j, half), :] == mine
                total = total + jnp.where(same, acts[pl.ds(at - j, half), :], 0.0) * taps[
                    pl.ds(j, 1), :
                ]
            conv[b, pl.ds(piece * half, half), :] = total.astype(BF)

    def hand_over(b):
        @pl.when(x == b)
        def _():
            regroup[b] = conv[b]

        @pl.when(x != b)
        def _():
            pltpu.make_async_remote_copy(
                src_ref=conv.at[b],
                dst_ref=regroup.at[x],
                send_sem=c_send,
                recv_sem=c_recv,
                device_id=(sp, b),
                device_id_type=MESH,
            ).start()

    for b in range(1, NX):
        conv_block(b)

    peers = NX * CORES - 1 + 4

    @pl.when(sp < count - 1)
    def _():
        pl.semaphore_wait(barrier, peers + 1)

    @pl.when(sp == count - 1)
    def _():
        pl.semaphore_wait(barrier, peers)

    along_z(near_sem, (1, nz - 1))
    along_y(near_sem, (1, ny - 1))

    @pl.when(sp < count - 1)
    def _():
        for a in range(3):
            edge_copy(a).start()

    for b in range(1, NX):
        hand_over(b)
    start_weights((0,))
    pl.semaphore_wait(near_sem, 4)
    along_y(y_sem, range(1, ny))
    along_z(reach_sem, (1, 2, nz - 2, nz - 1))

    @pl.when(sp == 0)
    def _():
        acts[pl.ds(0, HALO), :] = jnp.zeros((HALO, LANES), F32)
        docsb[pl.ds(0, HALO), :] = jnp.full((HALO, LANES), -1.0, F32)

    @pl.when(sp > 0)
    def _():
        for a in range(3):
            edge_copy(a).wait_recv()
        acts[pl.ds(0, HALO), :] = gated(halo_v[...], halo_g[...])
        docsb[pl.ds(0, HALO), :] = spread(halo_d[pl.ds(NX - 1, 1), :])[LANES - HALO :]

    conv_block(0)
    hand_over(0)
    start_weights(range(1, 6))
    pl.semaphore_wait(y_sem, ny - 1)
    pl.semaphore_wait(reach_sem, 4)
    along_z(z_sem, range(1, nz))

    first = spread(ids[pl.ds(0, 1), :]) == lane.astype(F32)
    second = spread(ids[pl.ds(1, 1), :]) == lane.astype(F32)
    match = jnp.where(jnp.logical_or(first, second), 1.0, 0.0)
    rank = dot(jnp.where(lane < line, 1.0, 0.0).astype(BF), match.astype(BF))

    def column(row):
        return jnp.sum(jnp.where(line == lane, row, 0.0), axis=1, keepdims=True)

    gap = logits[pl.ds(0, 1), :] - logits[pl.ds(1, 1), :]
    w_first = column(prob[...] / (1.0 + jnp.exp(-gap)))
    w_second = column(prob[...] / (1.0 + jnp.exp(gap)))
    w_match = jnp.where(first, w_first, 0.0) + jnp.where(second, w_second, 0.0)
    picks = []
    for r in range(cap):
        at_rank = jnp.where(rank == float(r), match, 0.0)
        picks.append(at_rank.astype(BF))
        weight = at_rank * w_match
        high = weight.astype(BF)
        combine_w[pl.ds(0, block), pl.ds(r * LANES, LANES)] = high
        combine_w[pl.ds(block, block), pl.ds(r * LANES, LANES)] = (
            weight - high.astype(F32)
        ).astype(BF)

    pltpu.make_async_copy(
        regroup.at[pl.ds(0, NX - 1)], regroup.at[pl.ds(0, NX - 1)], c_recv
    ).wait()
    channels = NX * LANES
    parts = [regroup[b].astype(F32) for b in range(NX)]
    mean = jnp.sum(sum(parts[1:], parts[0]), axis=1, keepdims=True) / channels
    squares = [v * v for v in parts]
    square = jnp.sum(sum(squares[1:], squares[0]), axis=1, keepdims=True) / channels
    scale = lax.rsqrt(square - mean * mean + eps)
    for b in range(NX):
        cols = pl.ds(b * LANES, LANES)
        actv[:, cols] = silu((parts[b] - mean) * scale * gain[:, cols] + shift[:, cols]).astype(BF)
    load_ow.wait()
    load_stream.wait()
    summed = (stream_v[...].astype(F32) + dot(actv[...], ow_v[...])).astype(BF)
    resid[...] = summed
    wide = summed.astype(F32)
    power = jnp.sum(wide * wide, axis=1, keepdims=True) / width
    normed = (wide * lax.rsqrt(power + eps) * rms_gain[...]).astype(BF)

    for r in range(cap):
        rows_r = lax.dot_general(
            picks[r], normed, (((0,), (0,)), ((), ())), preferred_element_type=F32
        )
        for s in range(SUB):
            stage[pl.ds(s, experts, stride=SUB), :] = rows_r[:, s * LANES : (s + 1) * LANES]
        outg[:, r] = stage[...].astype(BF).reshape(experts, SUB, LANES)

    my_j = (x - member + NX) % NX
    my_e = ring * NX + my_j

    home = ny - 1
    own[home, core] = outg[my_e]

    def send_rows(g, carry):
        p = g // ny
        to_y = (y + g + 1) % ny
        for dz in spread_out(nz):
            base = ((z + dz) % nz) * ny + to_y
            for k in range(2):
                dd = 2 * p + (member + k) % 2
                j = (x - dd + NX) % NX
                m = ((dd + 1) // 2) % 2
                to_x = (j + m) % NX

                def start():
                    pltpu.make_async_remote_copy(
                        src_ref=outg.at[base * NX + j],
                        dst_ref=own.at[g, dz * CORES + core],
                        send_sem=a_send,
                        recv_sem=a_recv.at[g],
                        device_id=(base * CORES + seat(m, to_x), to_x),
                        device_id_type=MESH,
                    ).start()

                if dz == 0 and k == 0:
                    pl.when(g != home)(start)
                else:
                    start()
        return carry

    pl.semaphore_wait(z_sem, nz - 1)
    lax.fori_loop(0, chunks, send_rows, 0)

    mate_x = (x + 1 - 2 * member + NX) % NX
    mate = (ring * CORES + seat(1 - member, mate_x), mate_x)

    def forward(g):
        return pltpu.make_async_remote_copy(
            src_ref=own.at[g],
            dst_ref=par.at[g],
            send_sem=f_send.at[g],
            recv_sem=f_recv.at[g],
            device_id=mate,
            device_id_type=MESH,
        )

    def partial_copy(g):
        return pltpu.make_async_remote_copy(
            src_ref=psend.at[g],
            dst_ref=precv.at[g],
            send_sem=p_send.at[g],
            recv_sem=p_recv.at[g],
            device_id=mate,
            device_id_type=MESH,
        )

    def arrive(g):
        @pl.when(g == home)
        def _():
            part = own.at[home, pl.ds(0, per - 1)]
            pltpu.make_async_copy(part, part, a_recv.at[home]).wait()

        @pl.when(g != home)
        def _():
            pltpu.make_async_copy(own.at[g], own.at[g], a_recv.at[g]).wait()

        forward(g).start()

    def load_rows(buf, g, base):
        stage[pl.ds(0, rows * SUB), :] = buf[g].reshape(rows * SUB, LANES).astype(F32)
        for s in range(SUB):
            piece = stage[pl.ds(s, rows, stride=SUB), :]
            xbuf[pl.ds(base, rows), pl.ds(s * LANES, LANES)] = piece.astype(BF)

    def compute(g):
        load_rows(own, g, 0)
        forward(g).wait_recv()
        load_rows(par, g, rows)
        x_all = xbuf[pl.ds(0, 2 * rows), :]
        hidden = []
        for q in range(2):
            hidden.append((silu(dot(x_all, wg[q])) * dot(x_all, wu[q])).astype(BF))
        total = dot(hidden[0], wd[0]) + dot(hidden[1], wd[1])
        acc[g] = total[:rows]
        psend[g] = total[rows:].astype(BF)
        partial_copy(g).start()

    def finish(g):
        partial_copy(g).wait_recv()
        for s in range(SUB):
            cols = pl.ds(s * LANES, LANES)
            whole = acc[g, :, cols] + precv[g, :, cols].astype(F32)
            stage[pl.ds(s, rows, stride=SUB), :] = whole
        rsend[g] = stage[pl.ds(0, rows * SUB), :].astype(BF).reshape(per, cap, SUB, LANES)

        @pl.when(g == home)
        def _():
            ret[my_e] = rsend[home, core]

        dd = member + g // ny * (3 - 2 * member)
        t = (my_j + dd) % NX
        to_y = (y - g - 1 + chunks + ny) % ny
        for dz in spread_out(nz):
            to_z = (z - dz + nz) % nz
            for c in range(CORES):

                def start():
                    pltpu.make_async_remote_copy(
                        src_ref=rsend.at[g, dz * CORES + c],
                        dst_ref=ret.at[my_e],
                        send_sem=r_send,
                        recv_sem=r_recv,
                        device_id=(place(to_z, to_y, c), t),
                        device_id_type=MESH,
                    ).start()

                if dz == 0:
                    pl.when(jnp.logical_or(g != home, core != c))(start)
                else:
                    start()

    arrive(0)
    arrive(1)
    for s in range(2):
        for a in range(6):
            src, dst = weight_piece(0, a, s)
            pltpu.make_async_copy(src, dst, w_recv.at[s, a]).wait()

    def step(i, carry):
        @pl.when(jnp.logical_and(i > 1, i < chunks))
        def _():
            arrive(i)

        @pl.when(jnp.logical_and(i >= LAG, i < chunks + LAG))
        def _():
            compute(i - LAG)

        @pl.when(i >= END_LAG)
        def _():
            finish(i - END_LAG)

        return carry

    lax.fori_loop(0, chunks + END_LAG, step, 0)

    got = ret.at[pl.ds(0, experts - 1)]
    pltpu.make_async_copy(got, got, r_recv).wait()

    for r in range(cap):
        stage[...] = ret[:, r].reshape(experts * SUB, LANES).astype(F32)
        for s in range(SUB):
            xbuf[pl.ds(r * experts, experts), pl.ds(s * LANES, LANES)] = stage[
                pl.ds(s, experts, stride=SUB), :
            ].astype(BF)
    mixed = dot(combine_w[...], xbuf[...])
    out[...] = (resid[...].astype(F32) + (mixed[:block] + mixed[block:])).astype(BF)

    sent = outg.at[pl.ds(0, experts - 1)]
    pltpu.make_async_copy(sent, sent, a_send).wait()
    pltpu.make_async_copy(got, got, r_send).wait()
    left = conv.at[pl.ds(0, NX - 1)]
    pltpu.make_async_copy(left, left, c_send).wait()
    for g in range(chunks):
        forward(g).wait_send()
        partial_copy(g).wait_send()

    @pl.when(sp < count - 1)
    def _():
        for a in range(3):
            edge_copy(a).wait_send()

    for l in range(2):
        d, slot, to = weight_plan(l)

        @pl.when(d != member)
        def _():
            for a in range(6):
                weight_copy(l, a, slot, to).wait_send()


def spread_out(size):
    return sorted(range(size), key=lambda d: (-min(d, size - d), d))


def rows_of(conv):
    return conv.shape[1]


def body(
    ny,
    nz,
    stream,
    conv_value,
    conv_gate,
    doc_ids,
    conv_taps,
    conv_bias,
    chan_gain,
    chan_shift,
    out_weight,
    rms_gain,
    expert_ids,
    group_prob,
    route_logits,
    expert_gate,
    expert_up,
    expert_down,
):
    cap = 3
    tokens, width = stream.shape
    chunks = 2 * ny
    per = nz * CORES
    rows = per * cap
    experts = ny * nz * NX
    quarter = expert_gate.shape[2]
    channels = NX * LANES
    vmem = pl.BlockSpec(memory_space=pltpu.VMEM)
    hbm = pl.BlockSpec(memory_space=pl.ANY)
    dma = pltpu.SemaphoreType.DMA
    return pl.pallas_call(
        functools.partial(layer_kernel, ny, nz, cap),
        out_shape=jax.ShapeDtypeStruct((tokens, width), BF),
        in_specs=[hbm] * 16,
        out_specs=vmem,
        scratch_shapes=[
            pltpu.VMEM((NX * tokens, LANES), BF),
            pltpu.VMEM((NX * tokens, LANES), BF),
            pltpu.VMEM((NX, LANES), jnp.int32),
            pltpu.VMEM(conv_taps.shape, F32),
            pltpu.VMEM((1, LANES), F32),
            pltpu.VMEM((1, channels), F32),
            pltpu.VMEM((1, channels), F32),
            pltpu.VMEM((1, width), F32),
            pltpu.VMEM((2, LANES), jnp.int32),
            pltpu.VMEM((1, LANES), F32),
            pltpu.VMEM((2, LANES), F32),
            pltpu.VMEM((HALO, LANES), BF),
            pltpu.VMEM((HALO, LANES), BF),
            pltpu.VMEM((NX, LANES), jnp.int32),
            pltpu.VMEM((HALO + NX * tokens, LANES), F32),
            pltpu.VMEM((HALO + NX * tokens, LANES), F32),
            pltpu.VMEM((NX, tokens, LANES), BF),
            pltpu.VMEM((NX, tokens, LANES), BF),
            pltpu.VMEM((tokens, channels), BF),
            pltpu.VMEM((tokens, width), BF),
            pltpu.VMEM((channels, width), BF),
            pltpu.VMEM((tokens, width), BF),
            pltpu.VMEM((experts * SUB, LANES), F32),
            pltpu.VMEM((experts * cap, width), BF),
            pltpu.VMEM((2 * tokens, experts * cap), BF),
            pltpu.VMEM((experts, cap, SUB, LANES), BF),
            pltpu.VMEM((chunks, per, cap, SUB, LANES), BF),
            pltpu.VMEM((chunks, per, cap, SUB, LANES), BF),
            pltpu.VMEM((2, width, quarter), BF),
            pltpu.VMEM((2, width, quarter), BF),
            pltpu.VMEM((2, quarter, width), BF),
            pltpu.VMEM((chunks, rows, width), F32),
            pltpu.VMEM((chunks, rows, width), BF),
            pltpu.VMEM((chunks, rows, width), BF),
            pltpu.VMEM((chunks, per, cap, SUB, LANES), BF),
            pltpu.VMEM((experts, cap, SUB, LANES), BF),
            dma((11,)),
            pltpu.SemaphoreType.REGULAR,
            pltpu.SemaphoreType.REGULAR,
            pltpu.SemaphoreType.REGULAR,
            pltpu.SemaphoreType.REGULAR,
            dma((2,)),
            dma((3,)),
            dma((3,)),
            dma,
            dma,
            dma((2, 6)),
            dma((2, 6)),
            dma,
            dma((chunks,)),
            dma((chunks,)),
            dma((chunks,)),
            dma((chunks,)),
            dma((chunks,)),
            dma,
            dma,
        ],
        compiler_params=pltpu.CompilerParams(
            collective_id=0, has_side_effects=True, vmem_limit_bytes=60000 * 1024
        ),
    )(
        stream,
        conv_value,
        conv_gate,
        doc_ids.reshape(NX, LANES),
        conv_taps,
        conv_bias.reshape(1, LANES),
        chan_gain.reshape(1, channels),
        chan_shift.reshape(1, channels),
        out_weight,
        rms_gain.reshape(1, width),
        expert_ids.T,
        group_prob.reshape(1, LANES),
        route_logits.T,
        expert_gate,
        expert_up,
        expert_down,
    )


def solution(mesh):
    placed = (
        P(("sp", "tp"), None),
        P("sp", "tp"),
        P("sp", "tp"),
        P("sp"),
        P(None, "tp"),
        P("tp"),
        P(),
        P(),
        P(),
        P(),
        P(("sp", "tp"), None),
        P(("sp", "tp")),
        P(("sp", "tp"), None),
        P("sp", None, "tp"),
        P("sp", None, "tp"),
        P("sp", "tp", None),
    )
    ny = 4
    nz = mesh.shape["sp"] // (ny * CORES)
    return jax.shard_map(
        functools.partial(body, ny, nz),
        mesh=mesh,
        in_specs=placed,
        out_specs=P(("sp", "tp"), None),
        check_vma=False,
    )
```
